512 devices in a mesh: ep: 128 (over z, y, core), tp: 4 (over x).
Axes of the slice: x: 4, y: 8, z: 8, core: 2. Of those that a mesh axis runs over, the one named last changes fastest.
Arguments:
- resid: bfloat16 [2048, 2048], P('ep'), may hold values from -40 to 40
- queries: bfloat16 [2048, 1024], P('ep', 'tp'), may hold values from -146 to 146
- new_keys: bfloat16 [2048, 512], P('ep', 'tp'), may hold values from -6 to 6
- new_values: bfloat16 [2048, 512], P('ep', 'tp'), may hold values from -18 to 18
- key_cache: bfloat16 [2048, 4, 256, 128], P('ep', 'tp'), may hold values from -5 to 5
- value_cache: bfloat16 [2048, 4, 256, 128], P('ep', 'tp'), may hold values from -18 to 18
- cum_gate: float32 [2048, 8, 256], P('ep', 'tp'), may hold values from -256 to 0, as said below
- forget_logit: float32 [2048, 8], P('ep', 'tp'), may hold values from -6 to 6
- forget_bias: float32 [8], P('tp'), may hold values from -3 to 2
- lengths: int32 [2048], P('ep'), may hold values from 32 to 256
- out_weight: bfloat16 [1024, 2048], P('tp'), may hold values from -0.1875 to 0.1875
- norm_gain: float32 [2048], replicated, may hold values from 0.1 to 1.9
- mix_vector: bfloat16 [2048], replicated, may hold values from -0.125 to 0.125
- routes: int32 [2048, 2], P('ep'), may hold values from 0 to 31, all different within a row; in each aligned block of 16 rows (0 to 15, 16 to 31, ...) at most 2 rows name the same one
- route_weight: float32 [2048, 2], P('ep'), may hold values from 0.2 to 1
- expert_gate: bfloat16 [128, 2048, 768], P('ep', 'tp'), may hold values from -0.125 to 0.125
- expert_up: bfloat16 [128, 2048, 768], P('ep', 'tp'), may hold values from -0.125 to 0.125
- expert_down: bfloat16 [128, 768, 2048], P('ep', None, 'tp'), may hold values from -0.109375 to 0.109375
- dense_gate: bfloat16 [2048, 3072], P('tp', 'ep'), may hold values from -0.125 to 0.125
- dense_up: bfloat16 [2048, 3072], P('tp', 'ep'), may hold values from -0.125 to 0.125
- dense_down: bfloat16 [3072, 2048], P('ep', 'tp'), may hold values from -0.109375 to 0.109375
Outputs:
- layer_out: bfloat16 [2048, 2048], P('ep', 'tp')
The draws below stay inside these ranges and needn't reach their ends.
Inputs may be any that keep to these rules, and one draw needn't show every extreme that they name: `routes`: each row names 2 different experts; the rows of one index of ep name no expert more than 2 times. `cum_gate`: for positions below the sequence's length, the running sum of the log forget gates of positions 0 to p; it never rises along p.
All inputs are finite; a program needn't handle non-finite values.
Results may differ from the reference program's by a relative error of at most 0.0095.
Values may be sent and summed in bfloat16 or wider, within the bound.
A program may use at most 64 MiB of HBM per device.

```python
import math
import jax
import jax.numpy as jnp
import numpy as np
from jax import lax

D = 2048
QUERY_HEADS = 8
KV_HEADS = 4
HEAD = 128
FF = 3072
FFD = 3072
TOP_K = 2
EXP_SPAN = 4
SEQ_DEV = 16
CACHE_SLOTS = 256
SEQUENCE_TOTAL = 2048
EXPERTS = 32
CAP = 2
FF_SPAN = 768
N_EP = 128
N_TP = 4


def first_keys(key):
    return jnp.clip(jax.random.normal(jax.random.fold_in(key, 11), (SEQUENCE_TOTAL, KV_HEADS, HEAD), jnp.float32), -5.0, 5.0)


def draw_key_cache(key, part):
    leading = first_keys(key)
    others = jnp.clip(jax.random.normal(jax.random.fold_in(key, 12), (SEQUENCE_TOTAL, KV_HEADS, CACHE_SLOTS, HEAD), jnp.float32), -5.0, 5.0)
    full = others.at[:, :, 0, :].set(leading)
    return full.astype(jnp.bfloat16)


def draw_queries(key, part):
    base = jnp.clip(jax.random.normal(jax.random.fold_in(key, 15), (SEQUENCE_TOTAL, QUERY_HEADS, HEAD), jnp.float32), -5.0, 5.0)
    return base.reshape(SEQUENCE_TOTAL, QUERY_HEADS * HEAD).astype(jnp.bfloat16)


def draw_resid(key, part):
    block_index = jnp.arange(D) * N_TP // D
    rising = 3.0 ** (block_index.astype(jnp.float32) / max(N_TP - 1, 1))
    column = jnp.exp(jax.random.uniform(jax.random.fold_in(key, 21), (D,), jnp.float32, 0.0, math.log(3.0)))
    base = jnp.clip(jax.random.normal(jax.random.fold_in(key, 22), (SEQUENCE_TOTAL, D), jnp.float32), -4.0, 4.0)
    rowscale = jnp.exp(jax.random.uniform(jax.random.fold_in(key, 23), (SEQUENCE_TOTAL,), jnp.float32, math.log(0.3), math.log(3.0)))
    values = base * rowscale[:, None] * (column * rising)[None, :] / 3.0
    return jnp.clip(values, -40.0, 40.0).astype(jnp.bfloat16)


def draw_cum_gate(key, part):
    slow_share = 0.5
    slower_path = jax.random.uniform(jax.random.fold_in(key, 31), (SEQUENCE_TOTAL, QUERY_HEADS, 1), jnp.float32) < slow_share
    whole_loss = jnp.exp(jax.random.uniform(jax.random.fold_in(key, 32), (SEQUENCE_TOTAL, QUERY_HEADS, 1), jnp.float32, math.log(0.5), math.log(2.0)))
    fast_rate = jnp.exp(jax.random.uniform(jax.random.fold_in(key, 33), (SEQUENCE_TOTAL, QUERY_HEADS, 1), jnp.float32, math.log(0.01), math.log(1.0 / 30.0)))
    decay_rate = jnp.where(slower_path, whole_loss / CACHE_SLOTS, fast_rate)
    coarse_estimate = jax.random.uniform(jax.random.fold_in(key, 34), (SEQUENCE_TOTAL, QUERY_HEADS, CACHE_SLOTS), jnp.float32, 0.2, 1.8)
    quarter = jnp.exp(jax.random.uniform(jax.random.fold_in(key, 35), (SEQUENCE_TOTAL, QUERY_HEADS, 4), jnp.float32, math.log(0.5), math.log(2.0)))
    per_block_pass = jnp.repeat(quarter, CACHE_SLOTS // 4, axis=2)
    sudden_spike = jax.random.uniform(jax.random.fold_in(key, 36), (SEQUENCE_TOTAL, QUERY_HEADS, CACHE_SLOTS), jnp.float32) < 3.0 / CACHE_SLOTS
    dropped_amount = jnp.log(jax.random.uniform(jax.random.fold_in(key, 37), (SEQUENCE_TOTAL, QUERY_HEADS, CACHE_SLOTS), jnp.float32, 0.5, 0.8))
    decode_steps = -decay_rate * coarse_estimate * per_block_pass + jnp.where(sudden_spike & slower_path, dropped_amount, 0.0)
    return jnp.cumsum(decode_steps, axis=2).astype(jnp.float32)


def touch_ends(values, key, low, high):
    longest = values.shape.index(max(values.shape))
    spots = []
    for shift in (0, 1):
        where = [jax.random.randint(jax.random.fold_in(key, axis), (), 0, length) for axis, length in enumerate(values.shape)]
        where[longest] = (where[longest] + shift) % values.shape[longest]
        spots.append(tuple(where))
    return values.at[spots[0]].set(low).at[spots[1]].set(high)


def steps_of(key, dims, cuts, smallest, high):
    def one(dim, shards_of):
        draws = jax.random.uniform(jax.random.fold_in(jax.random.fold_in(key, 6), dim), (shards_of,), jnp.float32, smallest / len(cuts), high / len(cuts))
        return jnp.repeat(jnp.exp(draws), dims[dim] // shards_of).reshape((-1,) + (1,) * (len(dims) - dim - 1))

    level = one(*cuts[0])
    for cut in cuts[1:]:
        level = level * one(*cut)
    return level


def shared_out(key, own, number, rows, number_of, top, most, lean):
    sequence = jax.random.permutation(key, number_of)
    crowded, usual = load_shares(number_of, rows * top, most, lean, True), load_shares(number_of, rows * top, most, lean, False)
    places = jnp.arange(number_of)

    def named(tallies, rotation):
        used = int((tallies > 0).sum())
        fixed = max(1, used // 4)
        moved = fixed + (places - fixed + rotation * (used - fixed)) % max(1, number_of - fixed)
        return jnp.zeros((number_of,), jnp.int32).at[sequence[jnp.where(places < fixed, places, moved)]].set(jnp.asarray(tallies, jnp.int32))

    tallies = jnp.where(number % 4 == 0, named(crowded, number // 4), named(usual, number - number // 4 - 1))
    mixed = jax.random.permutation(jax.random.fold_in(own, 3), number_of)
    giver, taker = mixed[0:number_of // 2 * 2:2], mixed[1:number_of // 2 * 2:2]
    slack = jnp.minimum(tallies[giver] - 1, most - tallies[taker]) // 2
    slack = jnp.where((giver == sequence[0]) | (taker == sequence[0]) | (tallies[taker] == 0), 0, jnp.maximum(slack, 0))
    moved = jax.random.randint(jax.random.fold_in(own, 4), (number_of // 2,), 0, 1 << 20) % (slack + 1)
    tallies = tallies.at[giver].add(-moved).at[taker].add(moved)
    labels = jnp.searchsorted(jnp.cumsum(tallies), jnp.arange(rows * top), side="right").astype(jnp.int32)
    listing = labels.reshape(top, rows).T
    listing = listing[jax.random.permutation(jax.random.fold_in(own, 1), rows)]
    rotation = jax.random.randint(jax.random.fold_in(own, 2), (rows, 1), 0, top)
    return jnp.take_along_axis(listing, (jnp.arange(top)[None, :] + rotation) % top, axis=1)


def load_shares(amount, total, reach, skew, full):
    loads = [(1 << 20) // math.isqrt(rank ** skew) + 1 for rank in range(1, amount + 1)]
    largest = reach if full else min(reach, max(-(-total // amount), total * loads[0] // sum(loads)))
    least = 1 if total - largest >= amount - 1 else 0
    counts, spare = [largest] + [least] * (amount - 1), total - largest - least * (amount - 1)
    while spare > 0:
        candidates = [i for i in range(1, amount) if counts[i] < largest] or [i for i in range(1, amount) if counts[i] < reach]
        mass, left = sum([loads[i] for i in candidates]), spare
        for i in candidates:
            addition = min(reach - counts[i], max(1, left * loads[i] // mass), spare)
            counts[i] = counts[i] + addition
            spare = spare - addition
    return np.array(counts)


def normal_values(key, dims, deviation, limit, cuts=(), held_as=jnp.bfloat16):
    values = jax.random.normal(key, dims, jnp.float32) * deviation
    if len(cuts) > 0:
        values = steps_of(key, dims, cuts, -0.22, 0.18) * values
    return jnp.clip(values, min=-limit, max=limit).astype(held_as)


def setup_inputs(seed: int = 0) -> dict:
    seeds = jax.random.split(jax.random.key(seed), 22)
    resid = draw_resid(jax.random.fold_in(seeds[21], 71), 0)
    queries = draw_queries(jax.random.fold_in(seeds[21], 71), 0)
    new_keys = normal_values(seeds[2], (SEQUENCE_TOTAL, KV_HEADS * HEAD), 1.0, 6.0, ((0, 128), (1, 4)))
    new_values = normal_values(seeds[3], (SEQUENCE_TOTAL, KV_HEADS * HEAD), 3.0, 18.0, ((0, 128), (1, 4)))
    key_cache = draw_key_cache(jax.random.fold_in(seeds[21], 71), 0)
    value_cache = normal_values(seeds[5], (SEQUENCE_TOTAL, KV_HEADS, CACHE_SLOTS, HEAD), 3.0, 18.0, ((0, 128), (1, 4)))
    cum_gate = draw_cum_gate(jax.random.fold_in(seeds[21], 71), 0)
    forget_logit = normal_values(seeds[7], (SEQUENCE_TOTAL, QUERY_HEADS), 1.0, 6.0, ((0, 128), (1, 4)), jnp.float32)
    forget_bias = jnp.clip(-3.0 + 5.0 * jax.random.uniform(seeds[8], (QUERY_HEADS,), jnp.float32) ** steps_of(seeds[8], (QUERY_HEADS,), ((0, 4),), -0.2, 0.2), -3.0, 2.0)
    lengths = touch_ends(jax.random.randint(seeds[9], (SEQUENCE_TOTAL,), CACHE_SLOTS // 8, CACHE_SLOTS + 1), jax.random.fold_in(seeds[9], 1), CACHE_SLOTS // 8, CACHE_SLOTS).astype(jnp.int32)
    out_weight = normal_values(seeds[10], (QUERY_HEADS * HEAD, D), (QUERY_HEADS * HEAD) ** -0.5, 0.1875, ((0, 4),))
    norm_gain = jnp.clip(1.0 + 0.18 * jax.random.normal(seeds[11], (D,), jnp.float32), 0.1, 1.9)
    mix_vector = normal_values(seeds[12], (D,), D ** -0.5, 0.125)
    routes_keys = jax.random.split(jax.random.fold_in(seeds[13], 1), SEQUENCE_TOTAL // SEQ_DEV)
    routes_turns = jax.random.permutation(jax.random.fold_in(seeds[13], 3), SEQUENCE_TOTAL // SEQ_DEV)
    routes = jax.vmap(lambda own, number: shared_out(jax.random.fold_in(seeds[13], 2), own, number, SEQ_DEV, EXPERTS, TOP_K, CAP, 1))(routes_keys, routes_turns).reshape((SEQUENCE_TOTAL, TOP_K))
    route_weight = jnp.clip(0.2 + 0.8 * jax.random.uniform(seeds[14], (SEQUENCE_TOTAL, TOP_K), jnp.float32) ** steps_of(seeds[14], (SEQUENCE_TOTAL, TOP_K), ((0, 128),), -0.2, 0.2), 0.2, 1.0)
    expert_gate = normal_values(seeds[15], (N_EP, D, FF_SPAN), D ** -0.5, 0.125, ((0, 128), (1, 4)))
    expert_up = normal_values(seeds[16], (N_EP, D, FF_SPAN), D ** -0.5, 0.125, ((0, 128), (1, 4)))
    expert_down = normal_values(seeds[17], (N_EP, FF_SPAN, D), FF ** -0.5, 0.109375, ((0, 128), (2, 4)))
    dense_gate = normal_values(seeds[18], (D, FFD), D ** -0.5, 0.125, ((0, 4), (1, 128)))
    dense_up = normal_values(seeds[19], (D, FFD), D ** -0.5, 0.125, ((0, 4), (1, 128)))
    dense_down = normal_values(seeds[20], (FFD, D), FFD ** -0.5, 0.109375, ((0, 128), (1, 4)))
    return dict(resid=resid, queries=queries, new_keys=new_keys, new_values=new_values, key_cache=key_cache, value_cache=value_cache, cum_gate=cum_gate, forget_logit=forget_logit, forget_bias=forget_bias, lengths=lengths, out_weight=out_weight, norm_gain=norm_gain, mix_vector=mix_vector, routes=routes, route_weight=route_weight, expert_gate=expert_gate, expert_up=expert_up, expert_down=expert_down, dense_gate=dense_gate, dense_up=dense_up, dense_down=dense_down)


EPSILON = 1e-06

def slot_table(route_block, expert_ids, capacity):
    blocks = route_block.shape[0]
    flat_routes = route_block.reshape(blocks, 1, -1)
    matched = (flat_routes == expert_ids.reshape(1, -1, 1)).astype(jnp.int32)
    ranking = jnp.cumsum(matched, axis=2) - 1
    slot_ids = jnp.arange(capacity, dtype=jnp.int32)
    taken = (matched[..., None] > 0) & (ranking[..., None] == slot_ids)
    table = jnp.swapaxes(taken, 2, 3).astype(jnp.float32)
    return table.reshape(blocks, expert_ids.shape[0], capacity, route_block.shape[1], route_block.shape[2])

def attend(queries, new_keys, new_values, key_cache, value_cache, cum_gate, forget_logit, forget_bias, lengths):
    seqcount = queries.shape[0]
    kv_local = key_cache.shape[1]
    grouping = QUERY_HEADS // KV_HEADS
    heads_local = kv_local * grouping
    scale_factor = 1.0 / math.sqrt(HEAD)
    query_float = queries.astype(jnp.float32).reshape(seqcount, kv_local, grouping, HEAD)
    scores = jnp.einsum('sgjd,sgpd->sgjp', query_float, key_cache.astype(jnp.float32))
    scores = scores.reshape(seqcount, heads_local, -1) * scale_factor
    own_score = jnp.einsum('sgjd,sgd->sgj', query_float, new_keys.astype(jnp.float32).reshape(seqcount, kv_local, HEAD))
    own_score = own_score.reshape(seqcount, heads_local) * scale_factor
    log_forget = jax.nn.log_sigmoid(forget_logit + forget_bias)
    position = jnp.arange(cum_gate.shape[2], dtype=jnp.int32)
    latest = lax.optimization_barrier(jnp.sum(jnp.where(position == (lengths - 1)[:, None, None], cum_gate, 0.0), axis=2))
    scores = scores + (latest + log_forget)[:, :, None] - cum_gate
    visible = position[None, None, :] < lengths[:, None, None]
    scores = jnp.where(visible, scores, -jnp.inf)
    highest = jnp.maximum(lax.optimization_barrier(jnp.max(scores, axis=2)), own_score)
    weights_past = jnp.exp(scores - highest[:, :, None])
    weight_own = jnp.exp(own_score - highest)
    totals = lax.optimization_barrier(jnp.sum(weights_past, axis=2)) + weight_own
    probs_past = (weights_past / totals[:, :, None]).astype(jnp.bfloat16)
    prob_own = (weight_own / totals).astype(jnp.bfloat16)
    mixed = jnp.einsum('sgjp,sgpd->sgjd', probs_past.astype(jnp.float32).reshape(seqcount, kv_local, grouping, -1), value_cache.astype(jnp.float32))
    mixed = mixed + prob_own.astype(jnp.float32).reshape(seqcount, kv_local, grouping, 1) * new_values.astype(jnp.float32).reshape(seqcount, kv_local, 1, HEAD)
    return mixed.reshape(seqcount, heads_local * HEAD).astype(jnp.bfloat16)

def reference(resid, queries, new_keys, new_values, key_cache, value_cache, cum_gate, forget_logit, forget_bias, lengths, out_weight, norm_gain, mix_vector, routes, route_weight, expert_gate, expert_up, expert_down, dense_gate, dense_up, dense_down):

    def per_block(pieces):
        q_block, k_new, v_new, k_cache, v_cache, gates_block, logit_block, length_block = pieces
        return attend(q_block, k_new, v_new, k_cache, v_cache, gates_block, logit_block, forget_bias, length_block)
    pieces = (queries.reshape(N_EP, SEQ_DEV, -1), new_keys.reshape(N_EP, SEQ_DEV, -1), new_values.reshape(N_EP, SEQ_DEV, -1), key_cache.reshape(N_EP, SEQ_DEV, KV_HEADS, CACHE_SLOTS, HEAD), value_cache.reshape(N_EP, SEQ_DEV, KV_HEADS, CACHE_SLOTS, HEAD), cum_gate.reshape(N_EP, SEQ_DEV, QUERY_HEADS, CACHE_SLOTS), forget_logit.reshape(N_EP, SEQ_DEV, QUERY_HEADS), lengths.reshape(N_EP, SEQ_DEV))
    attended = lax.map(per_block, pieces).reshape(SEQUENCE_TOTAL, QUERY_HEADS * HEAD)
    projected = jnp.dot(attended, out_weight, preferred_element_type=jnp.float32).astype(jnp.bfloat16)
    state = resid.astype(jnp.float32) + projected.astype(jnp.float32)
    inverse = lax.rsqrt(lax.optimization_barrier(jnp.mean(state * state, axis=1)) + EPSILON)
    normed = (state * inverse[:, None] * norm_gain).astype(jnp.bfloat16)
    gate = jax.nn.sigmoid(inverse * lax.optimization_barrier(jnp.sum(state * norm_gain * mix_vector.astype(jnp.float32), axis=1)))
    dense_g = jnp.dot(normed, dense_gate, preferred_element_type=jnp.float32)
    dense_u = jnp.dot(normed, dense_up, preferred_element_type=jnp.float32)
    dense_hidden = (jax.nn.silu(dense_g) * dense_u).astype(jnp.bfloat16)
    dense = jnp.dot(dense_hidden, dense_down, preferred_element_type=jnp.float32)
    route_block = routes.reshape(N_EP, SEQ_DEV, TOP_K)
    weight_block = route_weight.reshape(N_EP, SEQ_DEV, TOP_K)
    normed_block = normed.reshape(N_EP, SEQ_DEV, D).astype(jnp.float32)
    gate_blocks = expert_gate.reshape(EXPERTS, EXP_SPAN, D, FF_SPAN)
    up_blocks = expert_up.reshape(EXPERTS, EXP_SPAN, D, FF_SPAN)
    down_blocks = expert_down.reshape(EXPERTS, EXP_SPAN, FF_SPAN, D)

    def expert_step(total, inputs):
        expert_id, gate_part, up_part, down_part = inputs
        w_gate = jnp.transpose(gate_part, (1, 0, 2)).reshape(D, FF)
        w_up = jnp.transpose(up_part, (1, 0, 2)).reshape(D, FF)
        w_down = down_part.reshape(FF, D)
        table = slot_table(route_block, expert_id.reshape(1), CAP)[:, 0]
        picked = lax.optimization_barrier(jnp.sum(table, axis=3))
        chosen = jnp.einsum('bct,btd->bcd', picked, normed_block).astype(jnp.bfloat16).reshape(N_EP * CAP, D)
        gated = jnp.dot(chosen, w_gate, preferred_element_type=jnp.float32)
        upped = jnp.dot(chosen, w_up, preferred_element_type=jnp.float32)
        hidden = (jax.nn.silu(gated) * upped).astype(jnp.bfloat16)
        outputs = jnp.dot(hidden, w_down, preferred_element_type=jnp.float32).reshape(N_EP, CAP, D)
        share = jnp.einsum('bctk,btk,bcd->btd', table, weight_block, outputs, precision=lax.Precision.HIGHEST)
        return (total + share.reshape(SEQUENCE_TOTAL, D), None)
    routed, unused = lax.scan(expert_step, jnp.zeros((SEQUENCE_TOTAL, D), jnp.float32), (jnp.arange(EXPERTS, dtype=jnp.int32), gate_blocks, up_blocks, down_blocks))
    result = state + routed + gate[:, None] * dense
    return result.astype(jnp.bfloat16)
```

```python
import functools
import math

import jax
import jax.numpy as jnp
from jax import lax
from jax.experimental import pallas as pl
from jax.experimental.pallas import tpu as pltpu
from jax.sharding import PartitionSpec as P

HEAD = 128
EPSILON = 1e-06
NC = 2
NY = 8
F32 = jnp.float32
BF16 = jnp.bfloat16


def dot(a, b):
    return jnp.dot(a, b, preferred_element_type=F32)


def dot_t(a, b):
    return lax.dot_general(a, b, (((1,), (1,)), ((), ())), preferred_element_type=F32)


def kernel(
    dims,
    resid_ref,
    q_ref,
    nk_ref,
    nv_ref,
    bias_ref,
    codes_ref,
    gm_ref,
    k_hbm,
    v_hbm,
    wo_hbm,
    wg_hbm,
    wu_hbm,
    wd_hbm,
    dg_hbm,
    du_hbm,
    dd_hbm,
    out_ref,
    k_v,
    v_v,
    wo_v,
    wg_v,
    wu_v,
    wd_v,
    dg_v,
    du_v,
    dd_v,
    ct,
    dw,
    xbuf,
    st,
    rows,
    pk,
    wmat,
    disp,
    er,
    psend,
    prec,
    hid,
    dacc,
    ret,
    rb,
    csend,
    cb,
    lsem,
    x_s,
    x_r,
    c_s,
    c_r,
    w_s,
    w_r,
    y_s,
    y_r,
    f_s,
    f_r,
    z_s,
    z_r,
    g_s,
    g_r,
    p_s,
    p_r,
    h_s,
    h_r,
    o_s,
    o_r,
    b_s,
    b_r,
):
    NX, NZ, S, SLOTS, DX, CW, NCH, FD, FDP = dims
    NQ = NY * NC // 4
    ep = lax.axis_index("ep")
    t = lax.axis_index("tp")
    c = lax.rem(ep, NC)
    y = lax.rem(ep // NC, NY)
    z = ep // (NC * NY)
    q = y // 2
    o = 1 - c

    def dev(zz, yy, cc, xx):
        return ((zz * NY + yy) * NC + cc, xx)

    def remote(src, dst, ss, rs, where):
        d = pltpu.make_async_remote_copy(
            src_ref=src,
            dst_ref=dst,
            send_sem=ss,
            recv_sem=rs,
            device_id=where,
            device_id_type=pl.DeviceIdType.MESH,
        )
        d.start()
        sent.append(d)
        return d

    sent = []
    xs = [lax.rem(t + d, NX) for d in range(NX)]
    xb = [lax.rem(t + NX - d, NX) for d in range(NX)]
    ys = [lax.rem(y + d, NY) for d in range(NY)]
    yb = [lax.rem(y + NY - d, NY) for d in range(NY)]
    zs = [lax.rem(z + d, NZ) for d in range(NZ)]
    zb = [lax.rem(z + NZ - d, NZ) for d in range(NZ)]

    def order(n):
        return sorted(range(1, n), key=lambda d: (min(d, n - d), d))

    group = [(dc, dy) for dy in [0] + order(NY) for dc in range(NC) if dc + dy > 0]

    loads = {}
    for i, (name, src, dst) in enumerate(
        (
            ("dg", dg_hbm, dg_v),
            ("du", du_hbm, du_v),
            ("dd", dd_hbm, dd_v),
            ("k", k_hbm, k_v),
            ("v", v_hbm, v_v),
            ("wo", wo_hbm, wo_v),
            ("wg", wg_hbm, wg_v),
            ("wu", wu_hbm, wu_v),
            ("wd", wd_hbm, wd_v),
        )
    ):
        loads[name] = pltpu.make_async_copy(src, dst, lsem.at[i])
        loads[name].start()

    barrier = pltpu.get_barrier_semaphore()
    peers = [dev(z, y, c, xs[d]) for d in range(1, NX)]
    peers += [dev(z, ys[dy], (c if dc == 0 else o), t) for dc, dy in group]
    peers += [dev(zs[d], y, c, t) for d in range(1, NZ)]
    for p in peers:
        pl.semaphore_signal(barrier, inc=1, device_id=p, device_id_type=pl.DeviceIdType.MESH)

    loads["dg"].wait()
    loads["du"].wait()
    loads["dd"].wait()
    dw[z] = jnp.concatenate(
        [
            dg_v[...].astype(F32).T,
            du_v[...].astype(F32).T,
            dd_v[...].astype(F32),
            jnp.zeros((dw.shape[1] - 3 * FD, DX), F32),
        ],
        axis=0,
    ).astype(BF16)
    ct[c, y] = codes_ref[...]

    pl.semaphore_wait(barrier, len(peers))

    c_cp = {}
    for dc, dy in group:
        i = dc * NY + dy
        c_cp[i] = remote(
            codes_ref,
            ct.at[c, y],
            c_s.at[i],
            c_r.at[i],
            dev(z, ys[dy], (c if dc == 0 else o), t),
        )
    w_cp = {}
    for d in order(NZ):
        w_cp[d] = remote(dw.at[z], dw.at[z], w_s.at[d], w_r.at[d], dev(zs[d], y, c, t))

    loads["k"].wait()
    qq = q_ref[...]
    q2 = jnp.concatenate([qq[:, :HEAD], qq[:, HEAD:]], axis=0)
    rowid = lax.rem(lax.broadcasted_iota(jnp.int32, (2 * S, SLOTS), 0), S)
    raw = jnp.zeros((2 * S, SLOTS), F32)
    for s in range(S):
        part = dot_t(q2, k_v[s * SLOTS : (s + 1) * SLOTS, :])
        raw = jnp.where(rowid == s, part, raw)
    scale = 1.0 / math.sqrt(HEAD)
    scores = raw * scale + bias_ref[...]
    nk = nk_ref[...].astype(F32)
    nv = nv_ref[...].astype(F32)
    own = jnp.sum(q2.astype(F32) * jnp.concatenate([nk, nk], axis=0), axis=1, keepdims=True) * scale
    top = jnp.maximum(jnp.max(scores, axis=1, keepdims=True), own)
    past = jnp.exp(scores - top)
    wown = jnp.exp(own - top)
    total = jnp.sum(past, axis=1, keepdims=True) + wown
    probs = (past / total).astype(BF16).astype(F32)
    pown = (wown / total).astype(BF16).astype(F32)
    loads["v"].wait()
    mixed = pown * jnp.concatenate([nv, nv], axis=0)
    for s in range(S):
        mixed = mixed + dot(
            jnp.where(rowid == s, probs, 0.0).astype(BF16), v_v[s * SLOTS : (s + 1) * SLOTS, :]
        )
    mixed = mixed.astype(BF16)
    attended = jnp.concatenate([mixed[:S], mixed[S:]], axis=1)
    loads["wo"].wait()
    for j in range(NX):
        xbuf[t, j] = dot(attended, wo_v[:, j * DX : (j + 1) * DX]).astype(BF16)
    x_cp = {}
    for d in order(NX):
        x_cp[d] = remote(xbuf.at[t], xbuf.at[t], x_s.at[d], x_r.at[d], dev(z, y, c, xs[d]))

    for dc, dy in group:
        c_cp[dc * NY + dy].wait_recv()
    acode = [jnp.sum(ct[i], axis=0) for i in range(NC)]
    mine = jnp.sum(ct[c], axis=0)
    nslot = 2 * NY
    npick = NZ * nslot
    ntok = NY * S
    ii = lax.broadcasted_iota(jnp.int32, (npick, ntok), 0)
    tt = lax.broadcasted_iota(jnp.int32, (npick, ntok), 1)
    target = (2 * ((ii // nslot) * NQ + q) + lax.rem(ii // NY, 2) + 1).astype(F32)
    same = lax.rem(ii, NY) == tt // S
    hit = ((mine[0:1] == target) | (mine[1:2] == target)) & same
    pk[...] = jnp.where(hit, 1.0, 0.0).astype(BF16)
    nall = NC * npick
    ii = lax.broadcasted_iota(jnp.int32, (nall, NC * ntok), 0)
    tt = lax.broadcasted_iota(jnp.int32, (nall, NC * ntok), 1)
    target = (2 * ((ii // (NC * nslot)) * NQ + q) + lax.rem(ii // NY, 2) + 1).astype(F32)
    same = (lax.rem(ii, NY) == lax.rem(tt // S, NY)) & (lax.rem(ii // nslot, NC) == tt // ntok)
    allc = jnp.concatenate(acode, axis=1)
    wt = jnp.where((allc[0:1] == target) & same, allc[2:3], 0.0) + jnp.where(
        (allc[1:2] == target) & same, allc[3:4], 0.0
    )
    wt = wt.T
    whi = wt.astype(BF16)
    wmat[:, 0:nall] = whi
    wmat[:, nall : 2 * nall] = (wt - whi.astype(F32)).astype(BF16)

    for d in order(NX):
        x_cp[d].wait_recv()
    sumsq = jnp.zeros((S, 1), F32)
    gsum = jnp.zeros((S, 1), F32)
    for j in range(NX):
        proj = xbuf[0, j].astype(F32)
        for i in range(1, NX):
            proj = proj + xbuf[i, j].astype(F32)
        state = resid_ref[:, j * DX : (j + 1) * DX].astype(F32) + proj.astype(BF16).astype(F32)
        sumsq = sumsq + jnp.sum(state * state, axis=1, keepdims=True)
        scaled = state * gm_ref[0:1, j * DX : (j + 1) * DX]
        gsum = gsum + jnp.sum(scaled * gm_ref[1:2, j * DX : (j + 1) * DX], axis=1, keepdims=True)
        st[0, j] = state
        st[1, j] = scaled
    inverse = lax.rsqrt(sumsq / (NX * DX) + EPSILON)
    gate = 1.0 / (1.0 + jnp.exp(-(inverse * gsum)))
    ghi = gate.astype(BF16).astype(F32)
    lane = lax.broadcasted_iota(jnp.int32, (S, 128), 1)
    rows[c, y, :, 0:DX] = (st[1, t] * inverse).astype(BF16)
    rows[c, y, :, DX : DX + 128] = jnp.where(
        lane == 0, ghi, jnp.where(lane == 1, gate - ghi, 0.0)
    ).astype(BF16)

    y_cp, f_cp = {}, {}
    for d in order(NY):
        y_cp[d] = remote(
            rows.at[c, y], rows.at[c, y], y_s.at[d], y_r.at[d], dev(z, ys[d], c, t)
        )
    f_cp[0] = remote(rows.at[c, y], rows.at[c, y], f_s.at[0], f_r.at[0], dev(z, y, o, t))
    for d in order(NY):
        y_cp[d].wait_recv()
        f_cp[d] = remote(
            rows.at[c, yb[d]], rows.at[c, yb[d]], f_s.at[d], f_r.at[d], dev(z, y, o, t)
        )

    own_rows = rows[c, :, :, 0:DX].reshape(ntok, DX)
    disp[...] = dot(pk[...], own_rows).astype(BF16).reshape(NZ, nslot, DX)
    er[c * NZ + z] = disp[z]
    z_cp, g_cp = {}, {}
    for d in order(NZ):
        z_cp[d] = remote(
            disp.at[zs[d]], er.at[c * NZ + z], z_s.at[d], z_r.at[d], dev(zs[d], y, c, t)
        )
    g_cp[0] = remote(
        disp.at[z], er.at[c * NZ + z], g_s.at[0], g_r.at[0], dev(z, y, o, t)
    )

    for d in range(NY):
        f_cp[d].wait_recv()
    for d in order(NZ):
        w_cp[d].wait_recv()
    dwf = dw[...].astype(F32)
    fill = jnp.zeros((FDP - NZ * FD, DX), F32)
    dgw, duw, ddw = [
        jnp.concatenate([dwf[:, i * FD : (i + 1) * FD].reshape(NZ * FD, DX), fill], axis=0).astype(
            BF16
        )
        for i in range(3)
    ]
    ntoks = NC * ntok
    chunk = ntoks // NX
    all_rows = rows[:, :, :, 0:DX].reshape(ntoks, DX)
    psend[NCH, :, :, 0:CW] = dot_t(all_rows, dgw).astype(BF16).reshape(NX, chunk, CW)
    psend[NCH, :, :, CW : 2 * CW] = dot_t(all_rows, duw).astype(BF16).reshape(NX, chunk, CW)
    p_cp, h_cp = {}, {}

    def scatter(j):
        for d in order(NX)[::-1]:
            p_cp[j, d] = remote(
                psend.at[j, xs[d]],
                prec.at[j, d - 1],
                p_s.at[j, d - 1],
                p_r.at[j, d - 1],
                dev(z, y, c, xs[d]),
            )

    def hidden(j):
        acc = psend[j, t].astype(F32)
        for d in order(NX):
            p_cp[j, d].wait_recv()
        for d in range(1, NX):
            acc = acc + prec[j, d - 1].astype(F32)
        g, u = acc[:, :CW], acc[:, CW:]
        hid[j, t] = (g / (1.0 + jnp.exp(-g)) * u).astype(BF16)
        for d in order(NX)[::-1]:
            h_cp[j, d] = remote(
                hid.at[j, t],
                hid.at[j, t],
                h_s.at[j, d - 1],
                h_r.at[j, d - 1],
                dev(z, y, c, xs[d]),
            )

    def gathered(j):
        for d in order(NX):
            h_cp[j, d].wait_recv()
        return hid[j].reshape(ntoks, CW)

    scatter(NCH)

    for d in order(NZ):
        z_cp[d].wait_recv()
        g_cp[d] = remote(
            er.at[c * NZ + zb[d]],
            er.at[c * NZ + zb[d]],
            g_s.at[d],
            g_r.at[d],
            dev(z, y, o, t),
        )
    hidden(NCH)
    loads["wg"].wait()
    loads["wu"].wait()
    for d in range(NZ):
        g_cp[d].wait_recv()
    picked = er[...].reshape(nall, DX)
    for j in range(NCH):
        psend[j, :, :, 0:CW] = (
            dot(picked, wg_v[:, j * CW : (j + 1) * CW]).astype(BF16).reshape(NX, chunk, CW)
        )
        psend[j, :, :, CW : 2 * CW] = (
            dot(picked, wu_v[:, j * CW : (j + 1) * CW]).astype(BF16).reshape(NX, chunk, CW)
        )
        scatter(j)
    gates = rows[:, :, :, DX : DX + 128].reshape(ntoks, 128)
    gates = gates[:, 0:1].astype(F32) + gates[:, 1:2].astype(F32)
    dacc[...] = gates * dot(gathered(NCH), ddw)
    for j in range(NCH):
        hidden(j)
    loads["wd"].wait()
    outs = dot(gathered(0), wd_v[0:CW, :])
    for j in range(1, NCH):
        outs = outs + dot(gathered(j), wd_v[j * CW : (j + 1) * CW, :])
    outs = outs.astype(BF16)

    for zz in range(NZ):
        for cc in range(NC):
            at = (cc * NZ + zz) * nslot
            ret[zz, cc] = outs[at : at + nslot]
    rb[z] = ret[z]
    o_cp = {}
    for d in order(NZ)[::-1]:
        o_cp[d] = remote(ret.at[zs[d]], rb.at[z], o_s.at[d], o_r.at[d], dev(zs[d], y, c, t))
    for d in order(NZ):
        o_cp[d].wait_recv()
    back = rb[...].reshape(nall, DX)
    both = jnp.concatenate([back, back], axis=0)
    comb = dot(wmat[...], both) + dacc[...]
    csend[...] = comb.astype(BF16).reshape(NC, NY, S, DX)

    cb[c, y] = csend[c, y]
    b_cp = {}
    for dc, dy in group[::-1]:
        i = dc * NY + dy
        cc = c if dc == 0 else o
        b_cp[i] = remote(
            csend.at[cc, ys[dy]], cb.at[c, y], b_s.at[i], b_r.at[i], dev(z, ys[dy], cc, t)
        )
    for dc, dy in group:
        b_cp[dc * NY + dy].wait_recv()
    res = st[0, t]
    for cc in range(NC):
        for yy in range(NY):
            res = res + cb[cc, yy].astype(F32)
    out_ref[...] = res.astype(BF16)
    for d in sent:
        d.wait_send()


def body(
    resid,
    queries,
    new_keys,
    new_values,
    key_cache,
    value_cache,
    cum_gate,
    forget_logit,
    forget_bias,
    lengths,
    out_weight,
    norm_gain,
    mix_vector,
    routes,
    route_weight,
    expert_gate,
    expert_up,
    expert_down,
    dense_gate,
    dense_up,
    dense_down,
):
    NX = lax.axis_size("tp")
    n_ep = lax.axis_size("ep")
    NZ = n_ep // (NC * NY)
    S, D = resid.shape
    SLOTS = key_cache.shape[2]
    DX = D // NX
    FF = expert_gate.shape[2]
    FD = dense_gate.shape[1]
    CW = min(256, FF)
    NCH = FF // CW
    FDP = CW
    ep = lax.axis_index("ep")
    y = lax.rem(ep // NC, NY)

    position = jnp.arange(SLOTS, dtype=jnp.int32)
    lens = lengths[:, None, None]
    latest = jnp.sum(jnp.where(position == lens - 1, cum_gate, 0.0), axis=2)
    log_forget = jax.nn.log_sigmoid(forget_logit + forget_bias)
    bias = jnp.where(position < lens, (latest + log_forget)[:, :, None] - cum_gate, -jnp.inf)
    bias = jnp.swapaxes(bias, 0, 1).reshape(2 * S, SLOTS)

    earlier = jnp.arange(S)[None, :] < jnp.arange(S)[:, None]
    equal = routes[:, :, None, None] == routes[None, None, :, :]
    rank = jnp.sum(jnp.where(equal & earlier[:, None, :, None], 1, 0), axis=(2, 3))
    code = (2 * routes + rank + 1).astype(F32)
    four = jnp.concatenate([code.T, route_weight.T, jnp.zeros((4, S), F32)], axis=0)
    lane = jnp.arange(NY * S)
    codes = jnp.where(lane // S == y, jnp.tile(four, (1, NY)), 0.0)
    gm = jnp.stack([norm_gain, mix_vector.astype(F32)])

    dims = (NX, NZ, S, SLOTS, DX, CW, NCH, FD, FDP)
    nslot = 2 * NY
    npick = NZ * nslot
    ntok = NY * S
    DWR = -(-3 * FD // 16) * 16
    vm = pl.BlockSpec(memory_space=pltpu.VMEM)
    hb = pl.BlockSpec(memory_space=pl.ANY)
    dma = pltpu.SemaphoreType.DMA
    scratch = [
        pltpu.VMEM((S * SLOTS, HEAD), BF16),
        pltpu.VMEM((S * SLOTS, HEAD), BF16),
        pltpu.VMEM((2 * HEAD, D), BF16),
        pltpu.VMEM((DX, FF), BF16),
        pltpu.VMEM((DX, FF), BF16),
        pltpu.VMEM((FF, DX), BF16),
        pltpu.VMEM((DX, FD), BF16),
        pltpu.VMEM((DX, FD), BF16),
        pltpu.VMEM((FD, DX), BF16),
        pltpu.VMEM((NC, NY, 8, ntok), F32),
        pltpu.VMEM((NZ, DWR, DX), BF16),
        pltpu.VMEM((NX, NX, S, DX), BF16),
        pltpu.VMEM((2, NX, S, DX), F32),
        pltpu.VMEM((NC, NY, S, DX + 128), BF16),
        pltpu.VMEM((npick, ntok), BF16),
        pltpu.VMEM((NC * ntok, 2 * NC * npick), BF16),
        pltpu.VMEM((NZ, nslot, DX), BF16),
        pltpu.VMEM((NC * NZ, nslot, DX), BF16),
        pltpu.VMEM((NCH + 1, NX, NC * ntok // NX, 2 * CW), BF16),
        pltpu.VMEM((NCH + 1, NX - 1, NC * ntok // NX, 2 * CW), BF16),
        pltpu.VMEM((NCH + 1, NX, NC * ntok // NX, CW), BF16),
        pltpu.VMEM((NC * ntok, DX), F32),
        pltpu.VMEM((NZ, NC, nslot, DX), BF16),
        pltpu.VMEM((NZ, NC, nslot, DX), BF16),
        pltpu.VMEM((NC, NY, S, DX), BF16),
        pltpu.VMEM((NC, NY, S, DX), BF16),
        dma((9,)),
        dma((NX,)),
        dma((NX,)),
        dma((NC * NY,)),
        dma((NC * NY,)),
        dma((NZ,)),
        dma((NZ,)),
        dma((NY,)),
        dma((NY,)),
        dma((NY,)),
        dma((NY,)),
        dma((NZ,)),
        dma((NZ,)),
        dma((NZ,)),
        dma((NZ,)),
        dma((NCH + 1, NX - 1)),
        dma((NCH + 1, NX - 1)),
        dma((NCH + 1, NX - 1)),
        dma((NCH + 1, NX - 1)),
        dma((NZ,)),
        dma((NZ,)),
        dma((NC * NY,)),
        dma((NC * NY,)),
    ]
    return pl.pallas_call(
        functools.partial(kernel, dims),
        name="layer",
        out_shape=jax.ShapeDtypeStruct((S, DX), BF16),
        in_specs=[vm] * 7 + [hb] * 9,
        out_specs=vm,
        scratch_shapes=scratch,
        compiler_params=pltpu.CompilerParams(
            collective_id=0, has_side_effects=True, vmem_limit_bytes=56 * 1024 * 1024
        ),
    )(
        resid,
        queries,
        new_keys,
        new_values,
        bias,
        codes,
        gm,
        key_cache.reshape(S * SLOTS, HEAD),
        value_cache.reshape(S * SLOTS, HEAD),
        out_weight,
        expert_gate[0],
        expert_up[0],
        expert_down[0],
        dense_gate,
        dense_up,
        dense_down,
    )


def solution(mesh):
    return jax.shard_map(
        body,
        mesh=mesh,
        in_specs=(
            P("ep", None),
            P("ep", "tp"),
            P("ep", "tp"),
            P("ep", "tp"),
            P("ep", "tp", None, None),
            P("ep", "tp", None, None),
            P("ep", "tp", None),
            P("ep", "tp"),
            P("tp"),
            P("ep"),
            P("tp", None),
            P(),
            P(),
            P("ep", None),
            P("ep", None),
            P("ep", "tp", None),
            P("ep", "tp", None),
            P("ep", None, "tp"),
            P("tp", "ep"),
            P("tp", "ep"),
            P("ep", "tp"),
        ),
        out_specs=P("ep", "tp"),
        check_vma=False,
    )
```

```python
import functools
import math

import jax
import jax.numpy as jnp
from jax import lax
from jax.experimental import pallas as pl
from jax.experimental.pallas import tpu as pltpu
from jax.sharding import PartitionSpec as P

HEAD = 128
EPSILON = 1e-06
NC = 2
NY = 8
F32 = jnp.float32
BF16 = jnp.bfloat16


def dot(a, b):
    return jnp.dot(a, b, preferred_element_type=F32)


def dot_t(a, b):
    return lax.dot_general(a, b, (((1,), (1,)), ((), ())), preferred_element_type=F32)


ARGS = (
    ("resid", "q", "nk", "nv", "cg", "fl", "fb", "len", "rt", "rw", "gain", "mix")
    + ("k", "v", "wo", "wg", "wu", "wd", "dg", "du", "dd")
)


def kernel(dims, *refs):
    h = dict(zip(ARGS, refs))
    out_ref = refs[len(ARGS)]
    rest = refs[len(ARGS) + 1 :]
    local = dict(zip(ARGS[:18], rest))
    (codes, ct, dw, xbuf, st, rows, gts, pk, wmat, disp, er, psend, prec, hid) = rest[18:32]
    (psd, prd, hdd, dacc, osend, orecv, ret, rb, csend, cb) = rest[32:42]
    (lsem, xq, cq, wq, vq, yq, tq, zq, gq, pq, hq, aq, eq, sq, oq, bq) = rest[42:]
    NX, NZ, S, SLOTS, DX, CW, NCH, FD = dims
    NQ = NY * NC // 4
    ep = lax.axis_index("ep")
    t = lax.axis_index("tp")
    c = lax.rem(ep, NC)
    y = lax.rem(ep // NC, NY)
    z = ep // (NC * NY)
    q = y // 2
    o = 1 - c

    def dev(zz, yy, cc, xx):
        return ((zz * NY + yy) * NC + cc, xx)

    def remote(src, dst, sems, i, where):
        d = pltpu.make_async_remote_copy(
            src_ref=src,
            dst_ref=dst,
            send_sem=sems.at[(0, *i)],
            recv_sem=sems.at[(1, *i)],
            device_id=where,
            device_id_type=pl.DeviceIdType.MESH,
        )
        d.start()
        sent.append(d)
        return d

    sent = []
    xs = [lax.rem(t + d, NX) for d in range(NX)]
    xb = [lax.rem(t + NX - d, NX) for d in range(NX)]
    ys = [lax.rem(y + d, NY) for d in range(NY)]
    yb = [lax.rem(y + NY - d, NY) for d in range(NY)]
    zs = [lax.rem(z + d, NZ) for d in range(NZ)]
    zb = [lax.rem(z + NZ - d, NZ) for d in range(NZ)]

    def order(n):
        return sorted(range(1, n), key=lambda d: (min(d, n - d), d))

    partner = dev(z, y, o, t)
    barrier = pltpu.get_barrier_semaphore()
    peers = [dev(z, y, c, xs[d]) for d in range(1, NX)]
    peers += [dev(z, ys[d], c, t) for d in range(1, NY)]
    peers += [dev(zs[d], y, c, t) for d in range(1, NZ)]
    peers.append(partner)
    for p in peers:
        pl.semaphore_signal(barrier, inc=1, device_id=p, device_id_type=pl.DeviceIdType.MESH)

    loads = {}
    targets = dict(local, dg=dw.at[c, z, 0], du=dw.at[c, z, 1], dd=dw.at[c, z, 2])
    first = ["q", "k", "len", "rt", "cg", "fl", "fb", "rw", "nk", "nv", "v", "wo"]
    first += ["resid", "gain", "mix"]
    for i, name in enumerate(first + [a for a in ARGS if a not in first]):
        loads[name] = pltpu.make_async_copy(h[name], targets[name], lsem.at[i])
        loads[name].start()

    def get(name):
        loads[name].wait()
        return local[name]

    tr = lax.broadcasted_iota(jnp.int32, (S, S), 0)
    tc = lax.broadcasted_iota(jnp.int32, (S, S), 1)

    def column(row):
        return jnp.sum(jnp.where(tr == tc, row, jnp.zeros_like(row)), axis=1, keepdims=True)

    rt = get("rt")[...].astype(F32)
    rw = get("rw")[...]
    lanes = lax.broadcasted_iota(jnp.int32, (S, NY * S), 1)
    place = lanes == y * S + lax.broadcasted_iota(jnp.int32, (S, NY * S), 0)
    for k in range(2):
        mine = column(rt[k : k + 1])
        rank = jnp.zeros((S, 1), F32)
        for i in range(2):
            taken = (rt[i : i + 1] == mine) & (tc < tr)
            rank = rank + jnp.sum(jnp.where(taken, 1.0, 0.0), axis=1, keepdims=True)
        code = 2.0 * mine + rank + 1.0
        codes[k : k + 1] = jnp.sum(jnp.where(place, code, 0.0), axis=0, keepdims=True)
        codes[2 + k : 3 + k] = jnp.sum(
            jnp.where(place, column(rw[k : k + 1]), 0.0), axis=0, keepdims=True
        )
    codes[4:8] = jnp.zeros((4, NY * S), F32)
    ct[y] = codes[...]

    lens = column(get("len")[...])
    cg_ref, fl_ref, fb_ref = get("cg"), get("fl"), get("fb")
    pos = lax.broadcasted_iota(jnp.int32, (S, SLOTS), 1)
    biases = []
    for j in range(2):
        cg = cg_ref[:, j, :]
        latest = jnp.sum(jnp.where(pos == lens - 1, cg, 0.0), axis=1, keepdims=True)
        pre = column(fl_ref[j : j + 1]) + fb_ref[0:1, j : j + 1]
        forget = jnp.minimum(pre, 0.0) - jnp.log(1.0 + jnp.exp(-jnp.abs(pre)))
        biases.append(jnp.where(pos < lens, latest + forget - cg, -jnp.inf))
    bias = jnp.concatenate(biases, axis=0)

    k_v = get("k")
    qq = get("q")[...]
    q2 = jnp.concatenate([qq[:, :HEAD], qq[:, HEAD:]], axis=0)
    rowid = lax.rem(lax.broadcasted_iota(jnp.int32, (2 * S, SLOTS), 0), S)
    raw = jnp.zeros((2 * S, SLOTS), F32)
    for s in range(S):
        part = dot_t(q2, k_v[s * SLOTS : (s + 1) * SLOTS, :])
        raw = jnp.where(rowid == s, part, raw)
    scale = 1.0 / math.sqrt(HEAD)
    scores = raw * scale + bias
    nk = get("nk")[...].astype(F32)
    nv = get("nv")[...].astype(F32)
    own = jnp.sum(q2.astype(F32) * jnp.concatenate([nk, nk], axis=0), axis=1, keepdims=True) * scale
    top = jnp.maximum(jnp.max(scores, axis=1, keepdims=True), own)
    past = jnp.exp(scores - top)
    wown = jnp.exp(own - top)
    total = jnp.sum(past, axis=1, keepdims=True) + wown
    probs = (past / total).astype(BF16).astype(F32)
    pown = (wown / total).astype(BF16).astype(F32)
    v_v = get("v")
    mixed = pown * jnp.concatenate([nv, nv], axis=0)
    for s in range(S):
        mixed = mixed + dot(
            jnp.where(rowid == s, probs, 0.0).astype(BF16), v_v[s * SLOTS : (s + 1) * SLOTS, :]
        )
    mixed = mixed.astype(BF16)
    attended = jnp.concatenate([mixed[:S], mixed[S:]], axis=1)
    wo_v = get("wo")
    for j in range(NX):
        xbuf[t, j] = dot(attended, wo_v[:, j * DX : (j + 1) * DX]).astype(BF16)
    pl.semaphore_wait(barrier, len(peers))
    x_cp, c_cp, w_cp = {}, {}, {}
    for d in order(NX):
        x_cp[d] = remote(xbuf.at[t], xbuf.at[t], xq, (d,), dev(z, y, c, xs[d]))
    for d in order(NY):
        c_cp[d] = remote(codes, ct.at[y], cq, (d,), dev(z, ys[d], c, t))
    for name in ("dg", "du", "dd"):
        loads[name].wait()
    for d in order(NZ):
        w_cp[d] = remote(dw.at[c, z], dw.at[c, z], wq, (d,), dev(zs[d], y, c, t))

    for d in order(NY):
        c_cp[d].wait_recv()
    mine = jnp.sum(ct[...], axis=0)
    nslot = 2 * NY
    npick = NZ * nslot
    ntok = NY * S
    ii = lax.broadcasted_iota(jnp.int32, (npick, ntok), 0)
    tt = lax.broadcasted_iota(jnp.int32, (npick, ntok), 1)
    target = (2 * ((ii // nslot) * NQ + q) + lax.rem(ii // NY, 2) + 1).astype(F32)
    same = lax.rem(ii, NY) == tt // S
    hits = [(mine[k : k + 1] == target) & same for k in range(2)]
    pk[...] = jnp.where(hits[0] | hits[1], 1.0, 0.0).astype(BF16)
    wt = jnp.where(hits[0], mine[2:3], 0.0) + jnp.where(hits[1], mine[3:4], 0.0)
    wt = wt.T
    whi = wt.astype(BF16)
    wmat[:, 0:npick] = whi
    wmat[:, npick : 2 * npick] = (wt - whi.astype(F32)).astype(BF16)

    resid_ref, gain_ref, mix_ref = get("resid"), get("gain"), get("mix")
    def row_of(ref, j):
        n = DX // 128
        return jnp.concatenate(
            [ref[j * n + i : j * n + i + 1, :].astype(F32) for i in range(n)], axis=1
        )

    for d in order(NX):
        x_cp[d].wait_recv()
    sumsq = jnp.zeros((S, 1), F32)
    gsum = jnp.zeros((S, 1), F32)
    for j in range(NX):
        proj = xbuf[0, j].astype(F32)
        for i in range(1, NX):
            proj = proj + xbuf[i, j].astype(F32)
        state = resid_ref[:, j * DX : (j + 1) * DX].astype(F32) + proj.astype(BF16).astype(F32)
        sumsq = sumsq + jnp.sum(state * state, axis=1, keepdims=True)
        scaled = state * row_of(gain_ref, j)
        gsum = gsum + jnp.sum(scaled * row_of(mix_ref, j), axis=1, keepdims=True)
        st[0, j] = state
        st[1, j] = scaled
    inverse = lax.rsqrt(sumsq / (NX * DX) + EPSILON)
    gate = 1.0 / (1.0 + jnp.exp(-(inverse * gsum)))
    ghi = gate.astype(BF16).astype(F32)
    lane = lax.broadcasted_iota(jnp.int32, (S, 128), 1)
    rows[y] = (st[1, t] * inverse).astype(BF16)
    gts[y] = jnp.where(lane == 0, ghi, jnp.where(lane == 1, gate - ghi, 0.0)).astype(BF16)

    y_cp, t_cp = {}, {}
    for d in order(NY):
        y_cp[d] = remote(rows.at[y], rows.at[y], yq, (d,), dev(z, ys[d], c, t))
    for d in order(NY):
        t_cp[d] = remote(gts.at[y], gts.at[y], tq, (d,), dev(z, ys[d], c, t))
    for d in order(NY):
        y_cp[d].wait_recv()

    own_rows = rows[...].reshape(ntok, DX)
    disp[...] = dot(pk[...], own_rows).astype(BF16).reshape(NZ, nslot, DX)
    er[c, z] = disp[z]
    z_cp, g_cp = {}, {}
    for d in order(NZ):
        z_cp[d] = remote(disp.at[zs[d]], er.at[c, z], zq, (d,), dev(zs[d], y, c, t))
    g_cp[0] = remote(disp.at[z], er.at[c, z], gq, (0,), partner)

    for d in order(NZ):
        w_cp[d].wait_recv()
    v_cp = remote(dw.at[c], dw.at[c], vq, (0,), partner)
    v_cp.wait_recv()

    nden = NC * NZ * FD
    dgw, duw, ddw = [
        dw[:, :, i].astype(F32).reshape(nden, DX).astype(BF16) for i in range(3)
    ]
    dchunk = ntok // NX
    psd[:, :, 0:nden] = dot_t(own_rows, dgw).astype(BF16).reshape(NX, dchunk, nden)
    psd[:, :, nden : 2 * nden] = dot_t(own_rows, duw).astype(BF16).reshape(NX, dchunk, nden)
    a_cp, e_cp = {}, {}
    for d in order(NX)[::-1]:
        a_cp[d] = remote(psd.at[xs[d]], prd.at[d - 1], aq, (d,), dev(z, y, c, xs[d]))
    nall = NC * npick
    chunk = nall // NX
    p_cp, h_cp = {}, {}

    def scatter(j):
        for d in order(NX)[::-1]:
            p_cp[j, d] = remote(
                psend.at[j, xs[d]],
                prec.at[j, d - 1],
                pq,
                (j, d - 1),
                dev(z, y, c, xs[d]),
            )

    def hidden(j):
        acc = psend[j, t].astype(F32)
        for d in order(NX):
            p_cp[j, d].wait_recv()
        for d in range(1, NX):
            acc = acc + prec[j, d - 1].astype(F32)
        hid[j, t] = swish(acc, CW)
        for d in order(NX)[::-1]:
            h_cp[j, d] = remote(
                hid.at[j, t], hid.at[j, t], hq, (j, d - 1), dev(z, y, c, xs[d])
            )

    def swish(acc, n):
        g, u = acc[:, :n], acc[:, n:]
        return (g / (1.0 + jnp.exp(-g)) * u).astype(BF16)

    for d in order(NZ):
        z_cp[d].wait_recv()
        g_cp[d] = remote(er.at[c, zb[d]], er.at[c, zb[d]], gq, (d,), partner)
    acc = psd[t].astype(F32)
    for d in order(NX):
        a_cp[d].wait_recv()
        acc = acc + prd[d - 1].astype(F32)
    hdd[t] = swish(acc, nden)
    for d in order(NX)[::-1]:
        e_cp[d] = remote(hdd.at[t], hdd.at[t], eq, (d,), dev(z, y, c, xs[d]))
    wg_v, wu_v = get("wg"), get("wu")
    for d in range(NZ):
        g_cp[d].wait_recv()
    picked = er[...].reshape(nall, DX)
    for j in range(NCH):
        psend[j, :, :, 0:CW] = (
            dot(picked, wg_v[:, j * CW : (j + 1) * CW]).astype(BF16).reshape(NX, chunk, CW)
        )
        psend[j, :, :, CW : 2 * CW] = (
            dot(picked, wu_v[:, j * CW : (j + 1) * CW]).astype(BF16).reshape(NX, chunk, CW)
        )
        scatter(j)
    for d in order(NY):
        t_cp[d].wait_recv()
    for d in order(NX):
        e_cp[d].wait_recv()
    gates = gts[...].reshape(ntok, 128)
    gates = gates[:, 0:1].astype(F32) + gates[:, 1:2].astype(F32)
    dacc[...] = gates * dot(hdd[...].reshape(ntok, nden), ddw)
    for j in range(NCH):
        hidden(j)
    wd_v = get("wd")
    half = NX // NC

    def down(which, j):
        rows_in = hid[j, pl.ds(which * half, half)].reshape(npick, CW)
        return dot(rows_in, wd_v[j * CW : (j + 1) * CW, :])

    for j in range(NCH):
        for d in order(NX):
            h_cp[j, d].wait_recv()
        if j == 0:
            theirs, ours = down(o, 0), down(c, 0)
        elif j < NCH - 1:
            theirs, ours = theirs + down(o, j), ours + down(c, j)
    if NCH > 1:
        theirs = theirs + down(o, NCH - 1)

    osend[...] = theirs.astype(BF16).reshape(NZ, nslot, DX)
    s_cp = remote(osend, orecv, sq, (0,), partner)
    if NCH > 1:
        ours = ours + down(c, NCH - 1)
    s_cp.wait_recv()
    ret[...] = (ours + orecv[...].reshape(npick, DX).astype(F32)).astype(BF16).reshape(
        NZ, nslot, DX
    )

    o_cp = {}
    for d in order(NZ)[::-1]:
        o_cp[d] = remote(ret.at[zs[d]], rb.at[z], oq, (d,), dev(zs[d], y, c, t))
    rb[z] = ret[z]
    for d in order(NZ):
        o_cp[d].wait_recv()
    back = rb[...].reshape(npick, DX)
    both = jnp.concatenate([back, back], axis=0)
    comb = dot(wmat[...], both) + dacc[...]
    csend[...] = comb.astype(BF16).reshape(NY, S, DX)

    b_cp = {}
    for d in order(NY)[::-1]:
        b_cp[d] = remote(csend.at[ys[d]], cb.at[y], bq, (d,), dev(z, ys[d], c, t))
    cb[y] = csend[y]
    for d in order(NY):
        b_cp[d].wait_recv()
    res = st[0, t]
    for yy in range(NY):
        res = res + cb[yy].astype(F32)
    out_ref[...] = res.astype(BF16)
    for d in sent:
        d.wait_send()


def body(
    resid,
    queries,
    new_keys,
    new_values,
    key_cache,
    value_cache,
    cum_gate,
    forget_logit,
    forget_bias,
    lengths,
    out_weight,
    norm_gain,
    mix_vector,
    routes,
    route_weight,
    expert_gate,
    expert_up,
    expert_down,
    dense_gate,
    dense_up,
    dense_down,
):
    NX = lax.axis_size("tp")
    n_ep = lax.axis_size("ep")
    NZ = n_ep // (NC * NY)
    S, D = resid.shape
    SLOTS = key_cache.shape[2]
    DX = D // NX
    FF = expert_gate.shape[2]
    FD = dense_gate.shape[1]
    CW = min(256, FF)
    NCH = FF // CW
    dims = (NX, NZ, S, SLOTS, DX, CW, NCH, FD)
    nslot = 2 * NY
    npick = NZ * nslot
    ntok = NY * S
    nden = NC * NZ * FD
    chunk = NC * npick // NX
    dchunk = ntok // NX
    vm = pl.BlockSpec(memory_space=pltpu.VMEM)
    hb = pl.BlockSpec(memory_space=pl.ANY)
    args = (
        resid,
        queries,
        new_keys,
        new_values,
        cum_gate,
        forget_logit.T,
        forget_bias.reshape(1, 2),
        lengths.reshape(1, S),
        routes.T,
        route_weight.T,
        norm_gain.reshape(D // 128, 128),
        mix_vector.reshape(D // 128, 128),
        key_cache.reshape(S * SLOTS, HEAD),
        value_cache.reshape(S * SLOTS, HEAD),
        out_weight,
        expert_gate[0],
        expert_up[0],
        expert_down[0],
        dense_gate.T,
        dense_up.T,
        dense_down,
    )
    scratch = [pltpu.VMEM(a.shape, a.dtype) for a in args[:18]]
    scratch += [
        pltpu.VMEM(*sd)
        for sd in (
            ((8, ntok), F32),
            ((NY, 8, ntok), F32),
            ((NC, NZ, 3, FD, DX), BF16),
            ((NX, NX, S, DX), BF16),
            ((2, NX, S, DX), F32),
            ((NY, S, DX), BF16),
            ((NY, S, 128), BF16),
            ((npick, ntok), BF16),
            ((ntok, 2 * npick), BF16),
            ((NZ, nslot, DX), BF16),
            ((NC, NZ, nslot, DX), BF16),
            ((NCH, NX, chunk, 2 * CW), BF16),
            ((NCH, NX - 1, chunk, 2 * CW), BF16),
            ((NCH, NX, chunk, CW), BF16),
            ((NX, dchunk, 2 * nden), BF16),
            ((NX - 1, dchunk, 2 * nden), BF16),
            ((NX, dchunk, nden), BF16),
            ((ntok, DX), F32),
            ((NZ, nslot, DX), BF16),
            ((NZ, nslot, DX), BF16),
            ((NZ, nslot, DX), BF16),
            ((NZ, nslot, DX), BF16),
            ((NY, S, DX), BF16),
            ((NY, S, DX), BF16),
        )
    ]
    dma = pltpu.SemaphoreType.DMA
    scratch += [dma((len(args),))]
    scratch += [
        dma((2, *n))
        for n in (
            (NX,),
            (NY,),
            (NZ,),
            (1,),
            (NY,),
            (NY,),
            (NZ,),
            (NZ,),
            (NCH, NX - 1),
            (NCH, NX - 1),
            (NX,),
            (NX,),
            (1,),
            (NZ,),
            (NY,),
        )
    ]
    return pl.pallas_call(
        functools.partial(kernel, dims),
        name="layer",
        out_shape=pltpu.VMEM((S, DX), BF16),
        in_specs=[hb] * len(args),
        out_specs=vm,
        scratch_shapes=scratch,
        compiler_params=pltpu.CompilerParams(
            collective_id=0, has_side_effects=True, vmem_limit_bytes=56 * 1024 * 1024
        ),
    )(*args)


def solution(mesh):
    return jax.shard_map(
        body,
        mesh=mesh,
        in_specs=(
            P("ep", None),
            P("ep", "tp"),
            P("ep", "tp"),
            P("ep", "tp"),
            P("ep", "tp", None, None),
            P("ep", "tp", None, None),
            P("ep", "tp", None),
            P("ep", "tp"),
            P("tp"),
            P("ep"),
            P("tp", None),
            P(),
            P(),
            P("ep", None),
            P("ep", None),
            P("ep", "tp", None),
            P("ep", "tp", None),
            P("ep", None, "tp"),
            P("tp", "ep"),
            P("tp", "ep"),
            P("ep", "tp"),
        ),
        out_specs=P("ep", "tp"),
        check_vma=False,
    )
```

```python
import functools
import math

import jax
import jax.numpy as jnp
from jax import lax
from jax.experimental import pallas as pl
from jax.experimental.pallas import tpu as pltpu
from jax.sharding import PartitionSpec as P

HEAD = 128
EPSILON = 1e-06
NC = 2
NY = 8
F32 = jnp.float32
BF16 = jnp.bfloat16


def dot(a, b):
    return jnp.dot(a, b, preferred_element_type=F32)


def dot_t(a, b):
    return lax.dot_general(a, b, (((1,), (1,)), ((), ())), preferred_element_type=F32)


ARGS = (
    ("resid", "q", "nk", "nv", "cg", "fl", "fb", "len", "rt", "rw", "gain", "mix")
    + ("k", "v", "wo", "wg", "wu", "wd", "dg", "du", "dd")
)


def kernel(dims, *refs):
    h = dict(zip(ARGS, refs))
    out_ref = refs[len(ARGS)]
    rest = refs[len(ARGS) + 1 :]
    local = dict(zip(ARGS[:18], rest))
    (codes, ct, dw, xbuf, st, rows, gts, pk, wmat, disp, er, psend, prec, hid) = rest[18:32]
    (psd, prd, hdd, dacc, osend, orecv, ret, rb, csend, cb) = rest[32:42]
    (lsem, xq, cq, wq, vq, yq, tq, zq, gq, pq, hq, aq, eq, sq, oq, bq) = rest[42:]
    NX, NZ, S, SLOTS, DX, CW, NCH, FD = dims
    NQ = NY * NC // 4
    ep = lax.axis_index("ep")
    t = lax.axis_index("tp")
    c = lax.rem(ep, NC)
    y = lax.rem(ep // NC, NY)
    z = ep // (NC * NY)
    q = y // 2
    o = 1 - c

    def dev(zz, yy, cc, xx):
        return ((zz * NY + yy) * NC + cc, xx)

    def remote(src, dst, sems, i, where):
        d = pltpu.make_async_remote_copy(
            src_ref=src,
            dst_ref=dst,
            send_sem=sems.at[(0, *i)],
            recv_sem=sems.at[(1, *i)],
            device_id=where,
            device_id_type=pl.DeviceIdType.MESH,
        )
        d.start()
        sent.append(d)
        return d

    sent = []
    xs = [lax.rem(t + d, NX) for d in range(NX)]
    xb = [lax.rem(t + NX - d, NX) for d in range(NX)]
    ys = [lax.rem(y + d, NY) for d in range(NY)]
    yb = [lax.rem(y + NY - d, NY) for d in range(NY)]
    zs = [lax.rem(z + d, NZ) for d in range(NZ)]
    zb = [lax.rem(z + NZ - d, NZ) for d in range(NZ)]

    def order(n):
        return sorted(range(1, n), key=lambda d: (min(d, n - d), d))

    loads = {}
    targets = dict(local, dg=dw.at[c, z, 0], du=dw.at[c, z, 1], dd=dw.at[c, z, 2])
    first = ["q", "k", "len", "cg", "fl", "fb", "nk", "nv", "dg", "du", "dd", "v", "wo"]
    first += ["rt", "rw", "resid", "gain", "mix"]
    for i, name in enumerate(first + [a for a in ARGS if a not in first]):
        loads[name] = pltpu.make_async_copy(h[name], targets[name], lsem.at[i])
        loads[name].start()

    partner = dev(z, y, o, t)
    barrier = pltpu.get_barrier_semaphore()
    peers = [dev(z, y, c, xs[d]) for d in range(1, NX)]
    peers += [dev(z, ys[d], c, t) for d in range(1, NY)]
    peers += [dev(zs[d], y, c, t) for d in range(1, NZ)]
    peers.append(partner)
    for p in peers:
        pl.semaphore_signal(barrier, inc=1, device_id=p, device_id_type=pl.DeviceIdType.MESH)

    def get(name):
        loads[name].wait()
        return local[name]

    tr = lax.broadcasted_iota(jnp.int32, (S, S), 0)
    tc = lax.broadcasted_iota(jnp.int32, (S, S), 1)

    def column(row):
        return jnp.sum(jnp.where(tr == tc, row, jnp.zeros_like(row)), axis=1, keepdims=True)

    lens = column(get("len")[...])
    cg_ref, fl_ref, fb_ref = get("cg"), get("fl"), get("fb")
    pos = lax.broadcasted_iota(jnp.int32, (S, SLOTS), 1)
    biases = []
    for j in range(2):
        cg = cg_ref[:, j, :]
        latest = jnp.sum(jnp.where(pos == lens - 1, cg, 0.0), axis=1, keepdims=True)
        pre = column(fl_ref[j : j + 1]) + fb_ref[0:1, j : j + 1]
        forget = jnp.minimum(pre, 0.0) - jnp.log(1.0 + jnp.exp(-jnp.abs(pre)))
        biases.append(jnp.where(pos < lens, latest + forget - cg, -jnp.inf))
    bias = jnp.concatenate(biases, axis=0)

    k_v = get("k")
    qq = get("q")[...]
    q2 = jnp.concatenate([qq[:, :HEAD], qq[:, HEAD:]], axis=0)
    rowid = lax.rem(lax.broadcasted_iota(jnp.int32, (2 * S, SLOTS), 0), S)
    raw = jnp.zeros((2 * S, SLOTS), F32)
    for s in range(S):
        part = dot_t(q2, k_v[s * SLOTS : (s + 1) * SLOTS, :])
        raw = jnp.where(rowid == s, part, raw)
    scale = 1.0 / math.sqrt(HEAD)
    scores = raw * scale + bias
    nk = get("nk")[...].astype(F32)
    nv = get("nv")[...].astype(F32)
    own = jnp.sum(q2.astype(F32) * jnp.concatenate([nk, nk], axis=0), axis=1, keepdims=True) * scale
    top = jnp.maximum(jnp.max(scores, axis=1, keepdims=True), own)
    past = jnp.exp(scores - top)
    wown = jnp.exp(own - top)
    total = jnp.sum(past, axis=1, keepdims=True) + wown
    probs = (past / total).astype(BF16).astype(F32)
    pown = (wown / total).astype(BF16).astype(F32)
    pl.semaphore_wait(barrier, len(peers))
    for name in ("dg", "du", "dd"):
        loads[name].wait()
    near = [d for d in order(NZ) if min(d, NZ - d) <= 2]
    w_cp, v_cp = {}, {}
    for d in near:
        w_cp[d] = remote(dw.at[c, z], dw.at[c, z], wq, (d,), dev(zs[d], y, c, t))
    v_cp[0] = remote(dw.at[c, z], dw.at[c, z], vq, (0,), partner)

    def pass_on(d):
        w_cp[d].wait_recv()
        if d == NZ // 2 and NZ == 8:
            w_cp[4, 1].wait_recv()
        v_cp[d] = remote(dw.at[c, zb[d]], dw.at[c, zb[d]], vq, (d,), partner)

    v_v = get("v")
    mixed = pown * jnp.concatenate([nv, nv], axis=0)
    for s in range(S):
        mixed = mixed + dot(
            jnp.where(rowid == s, probs, 0.0).astype(BF16), v_v[s * SLOTS : (s + 1) * SLOTS, :]
        )
    mixed = mixed.astype(BF16)
    attended = jnp.concatenate([mixed[:S], mixed[S:]], axis=1)
    wo_v = get("wo")
    for j in range(NX):
        xbuf[t, j] = dot(attended, wo_v[:, j * DX : (j + 1) * DX]).astype(BF16)
    x_cp, c_cp = {}, {}
    for d in order(NX):
        x_cp[d] = remote(xbuf.at[t], xbuf.at[t], xq, (d,), dev(z, y, c, xs[d]))

    rt = get("rt")[...].astype(F32)
    rw = get("rw")[...]
    lanes = lax.broadcasted_iota(jnp.int32, (S, NY * S), 1)
    place = lanes == y * S + lax.broadcasted_iota(jnp.int32, (S, NY * S), 0)
    for k in range(2):
        mine = column(rt[k : k + 1])
        rank = jnp.zeros((S, 1), F32)
        for i in range(2):
            taken = (rt[i : i + 1] == mine) & (tc < tr)
            rank = rank + jnp.sum(jnp.where(taken, 1.0, 0.0), axis=1, keepdims=True)
        code = 2.0 * mine + rank + 1.0
        codes[k : k + 1] = jnp.sum(jnp.where(place, code, 0.0), axis=0, keepdims=True)
        codes[2 + k : 3 + k] = jnp.sum(
            jnp.where(place, column(rw[k : k + 1]), 0.0), axis=0, keepdims=True
        )
    codes[4:8] = jnp.zeros((4, NY * S), F32)
    ct[y] = codes[...]

    for d in order(NY):
        c_cp[d] = remote(codes, ct.at[y], cq, (d,), dev(z, ys[d], c, t))

    for d in order(NY):
        c_cp[d].wait_recv()
    mine = jnp.sum(ct[...], axis=0)
    nslot = 2 * NY
    npick = NZ * nslot
    ntok = NY * S
    ii = lax.broadcasted_iota(jnp.int32, (npick, ntok), 0)
    tt = lax.broadcasted_iota(jnp.int32, (npick, ntok), 1)
    target = (2 * ((ii // nslot) * NQ + q) + lax.rem(ii // NY, 2) + 1).astype(F32)
    same = lax.rem(ii, NY) == tt // S
    hits = [(mine[k : k + 1] == target) & same for k in range(2)]
    pk[...] = jnp.where(hits[0] | hits[1], 1.0, 0.0).astype(BF16)
    wt = jnp.where(hits[0], mine[2:3], 0.0) + jnp.where(hits[1], mine[3:4], 0.0)
    wt = wt.T
    whi = wt.astype(BF16)
    wmat[:, 0:npick] = whi
    wmat[:, npick : 2 * npick] = (wt - whi.astype(F32)).astype(BF16)

    resid_ref, gain_ref, mix_ref = get("resid"), get("gain"), get("mix")
    def row_of(ref, j):
        n = DX // 128
        return jnp.concatenate(
            [ref[j * n + i : j * n + i + 1, :].astype(F32) for i in range(n)], axis=1
        )

    for d in order(NX):
        x_cp[d].wait_recv()
    sumsq = jnp.zeros((S, 1), F32)
    gsum = jnp.zeros((S, 1), F32)
    for j in range(NX):
        proj = xbuf[0, j].astype(F32)
        for i in range(1, NX):
            proj = proj + xbuf[i, j].astype(F32)
        state = resid_ref[:, j * DX : (j + 1) * DX].astype(F32) + proj.astype(BF16).astype(F32)
        sumsq = sumsq + jnp.sum(state * state, axis=1, keepdims=True)
        scaled = state * row_of(gain_ref, j)
        gsum = gsum + jnp.sum(scaled * row_of(mix_ref, j), axis=1, keepdims=True)
        st[0, j] = state
        st[1, j] = scaled
    inverse = lax.rsqrt(sumsq / (NX * DX) + EPSILON)
    gate = 1.0 / (1.0 + jnp.exp(-(inverse * gsum)))
    ghi = gate.astype(BF16).astype(F32)
    lane = lax.broadcasted_iota(jnp.int32, (S, 128), 1)
    rows[y] = (st[1, t] * inverse).astype(BF16)
    gts[y] = jnp.where(lane == 0, ghi, jnp.where(lane == 1, gate - ghi, 0.0)).astype(BF16)

    y_cp, t_cp = {}, {}
    for d in order(NY):
        y_cp[d] = remote(rows.at[y], rows.at[y], yq, (d,), dev(z, ys[d], c, t))
    for d in order(NY):
        t_cp[d] = remote(gts.at[y], gts.at[y], tq, (d,), dev(z, ys[d], c, t))

    for d in near:
        pass_on(d)
    if NZ == 8:
        for d, to in ((2, 1), (6, 7)):
            f = (to + d) % NZ
            w_cp[f] = remote(
                dw.at[c, zb[d]], dw.at[c, zb[d]], wq, (f,), dev(zs[to], y, c, t)
            )
        for i, d in enumerate((2, 6)):
            part = (c, zb[d], slice(None), slice(None), pl.ds(i * (DX // 2), DX // 2))
            f = remote(dw.at[part], dw.at[part], wq, (4 * (1 - i),), dev(zs[d], y, c, t))
            w_cp[(4, 1) if i else 4] = f
    far = [d for d in order(NZ) if d not in near]
    for d in order(NY):
        y_cp[d].wait_recv()

    own_rows = rows[...].reshape(ntok, DX)
    disp[...] = dot(pk[...], own_rows).astype(BF16).reshape(NZ, nslot, DX)
    er[c, z] = disp[z]
    z_cp, g_cp = {}, {}
    for d in order(NZ):
        z_cp[d] = remote(disp.at[zs[d]], er.at[c, z], zq, (d,), dev(zs[d], y, c, t))
    g_cp[0] = remote(disp.at[z], er.at[c, z], gq, (0,), partner)

    for d in far:
        pass_on(d)

    for d in range(NZ):
        v_cp[d].wait_recv()

    nden = NC * NZ * FD
    dgw, duw, ddw = [
        dw[:, :, i].astype(F32).reshape(nden, DX).astype(BF16) for i in range(3)
    ]
    dchunk = ntok // NX
    psd[:, :, 0:nden] = dot_t(own_rows, dgw).astype(BF16).reshape(NX, dchunk, nden)
    psd[:, :, nden : 2 * nden] = dot_t(own_rows, duw).astype(BF16).reshape(NX, dchunk, nden)
    a_cp, e_cp = {}, {}
    for d in order(NX)[::-1]:
        a_cp[d] = remote(psd.at[xs[d]], prd.at[d - 1], aq, (d,), dev(z, y, c, xs[d]))
    nall = NC * npick
    chunk = nall // NX
    p_cp, h_cp = {}, {}

    def scatter(j):
        for d in order(NX)[::-1]:
            p_cp[j, d] = remote(
                psend.at[j, xs[d]],
                prec.at[j, d - 1],
                pq,
                (j, d - 1),
                dev(z, y, c, xs[d]),
            )

    def hidden(j):
        acc = psend[j, t].astype(F32)
        for d in order(NX):
            p_cp[j, d].wait_recv()
        for d in range(1, NX):
            acc = acc + prec[j, d - 1].astype(F32)
        hid[j, t] = swish(acc, CW)
        for d in order(NX)[::-1]:
            h_cp[j, d] = remote(
                hid.at[j, t], hid.at[j, t], hq, (j, d - 1), dev(z, y, c, xs[d])
            )

    def swish(acc, n):
        g, u = acc[:, :n], acc[:, n:]
        return (g / (1.0 + jnp.exp(-g)) * u).astype(BF16)

    for d in order(NZ):
        z_cp[d].wait_recv()
        g_cp[d] = remote(er.at[c, zb[d]], er.at[c, zb[d]], gq, (d,), partner)
    wg_v, wu_v = get("wg"), get("wu")
    for d in range(NZ):
        g_cp[d].wait_recv()
    picked = er[...].reshape(nall, DX)
    for j in range(NCH):
        psend[j, :, :, 0:CW] = (
            dot(picked, wg_v[:, j * CW : (j + 1) * CW]).astype(BF16).reshape(NX, chunk, CW)
        )
        psend[j, :, :, CW : 2 * CW] = (
            dot(picked, wu_v[:, j * CW : (j + 1) * CW]).astype(BF16).reshape(NX, chunk, CW)
        )
        scatter(j)
    for j in range(NCH):
        hidden(j)
    acc = psd[t].astype(F32)
    for d in order(NX):
        a_cp[d].wait_recv()
        acc = acc + prd[d - 1].astype(F32)
    hdd[t] = swish(acc, nden)
    for d in order(NX)[::-1]:
        e_cp[d] = remote(hdd.at[t], hdd.at[t], eq, (d,), dev(z, y, c, xs[d]))
    wd_v = get("wd")
    half = NX // NC

    def down(which, j):
        rows_in = hid[j, pl.ds(which * half, half)].reshape(npick, CW)
        return dot(rows_in, wd_v[j * CW : (j + 1) * CW, :])

    for j in range(NCH):
        for d in order(NX):
            h_cp[j, d].wait_recv()
        if j == 0:
            theirs, ours = down(o, 0), down(c, 0)
        elif j < NCH - 1:
            theirs, ours = theirs + down(o, j), ours + down(c, j)
    if NCH > 1:
        theirs = theirs + down(o, NCH - 1)

    osend[...] = theirs.astype(BF16).reshape(NZ, nslot, DX)
    s_cp = remote(osend, orecv, sq, (0,), partner)
    if NCH > 1:
        ours = ours + down(c, NCH - 1)
    s_cp.wait_recv()
    ret[...] = (ours + orecv[...].reshape(npick, DX).astype(F32)).astype(BF16).reshape(
        NZ, nslot, DX
    )

    o_cp = {}
    for d in order(NZ)[::-1]:
        o_cp[d] = remote(ret.at[zs[d]], rb.at[z], oq, (d,), dev(zs[d], y, c, t))
    rb[z] = ret[z]
    for d in order(NY):
        t_cp[d].wait_recv()
    for d in order(NX):
        e_cp[d].wait_recv()
    gates = gts[...].reshape(ntok, 128)
    gates = gates[:, 0:1].astype(F32) + gates[:, 1:2].astype(F32)
    dacc[...] = gates * dot(hdd[...].reshape(ntok, nden), ddw)
    for d in order(NZ):
        o_cp[d].wait_recv()
    back = rb[...].reshape(npick, DX)
    both = jnp.concatenate([back, back], axis=0)
    comb = dot(wmat[...], both) + dacc[...]
    csend[...] = comb.astype(BF16).reshape(NY, S, DX)

    b_cp = {}
    for d in order(NY)[::-1]:
        b_cp[d] = remote(csend.at[ys[d]], cb.at[y], bq, (d,), dev(z, ys[d], c, t))
    cb[y] = csend[y]
    for d in order(NY):
        b_cp[d].wait_recv()
    res = st[0, t]
    for yy in range(NY):
        res = res + cb[yy].astype(F32)
    out_ref[...] = res.astype(BF16)
    for d in sent:
        d.wait_send()


def body(
    resid,
    queries,
    new_keys,
    new_values,
    key_cache,
    value_cache,
    cum_gate,
    forget_logit,
    forget_bias,
    lengths,
    out_weight,
    norm_gain,
    mix_vector,
    routes,
    route_weight,
    expert_gate,
    expert_up,
    expert_down,
    dense_gate,
    dense_up,
    dense_down,
):
    NX = lax.axis_size("tp")
    n_ep = lax.axis_size("ep")
    NZ = n_ep // (NC * NY)
    S, D = resid.shape
    SLOTS = key_cache.shape[2]
    DX = D // NX
    FF = expert_gate.shape[2]
    FD = dense_gate.shape[1]
    CW = min(256, FF)
    NCH = FF // CW
    dims = (NX, NZ, S, SLOTS, DX, CW, NCH, FD)
    nslot = 2 * NY
    npick = NZ * nslot
    ntok = NY * S
    nden = NC * NZ * FD
    chunk = NC * npick // NX
    dchunk = ntok // NX
    vm = pl.BlockSpec(memory_space=pltpu.VMEM)
    hb = pl.BlockSpec(memory_space=pl.ANY)
    args = (
        resid,
        queries,
        new_keys,
        new_values,
        cum_gate,
        forget_logit.T,
        forget_bias.reshape(1, 2),
        lengths.reshape(1, S),
        routes.T,
        route_weight.T,
        norm_gain.reshape(D // 128, 128),
        mix_vector.reshape(D // 128, 128),
        key_cache.reshape(S * SLOTS, HEAD),
        value_cache.reshape(S * SLOTS, HEAD),
        out_weight,
        expert_gate[0],
        expert_up[0],
        expert_down[0],
        dense_gate.T,
        dense_up.T,
        dense_down,
    )
    scratch = [pltpu.VMEM(a.shape, a.dtype) for a in args[:18]]
    scratch += [
        pltpu.VMEM(*sd)
        for sd in (
            ((8, ntok), F32),
            ((NY, 8, ntok), F32),
            ((NC, NZ, 3, FD, DX), BF16),
            ((NX, NX, S, DX), BF16),
            ((2, NX, S, DX), F32),
            ((NY, S, DX), BF16),
            ((NY, S, 128), BF16),
            ((npick, ntok), BF16),
            ((ntok, 2 * npick), BF16),
            ((NZ, nslot, DX), BF16),
            ((NC, NZ, nslot, DX), BF16),
            ((NCH, NX, chunk, 2 * CW), BF16),
            ((NCH, NX - 1, chunk, 2 * CW), BF16),
            ((NCH, NX, chunk, CW), BF16),
            ((NX, dchunk, 2 * nden), BF16),
            ((NX - 1, dchunk, 2 * nden), BF16),
            ((NX, dchunk, nden), BF16),
            ((ntok, DX), F32),
            ((NZ, nslot, DX), BF16),
            ((NZ, nslot, DX), BF16),
            ((NZ, nslot, DX), BF16),
            ((NZ, nslot, DX), BF16),
            ((NY, S, DX), BF16),
            ((NY, S, DX), BF16),
        )
    ]
    dma = pltpu.SemaphoreType.DMA
    scratch += [dma((len(args),))]
    scratch += [
        dma((2, *n))
        for n in (
            (NX,),
            (NY,),
            (NZ,),
            (NZ,),
            (NY,),
            (NY,),
            (NZ,),
            (NZ,),
            (NCH, NX - 1),
            (NCH, NX - 1),
            (NX,),
            (NX,),
            (1,),
            (NZ,),
            (NY,),
        )
    ]
    return pl.pallas_call(
        functools.partial(kernel, dims),
        name="layer",
        out_shape=pltpu.VMEM((S, DX), BF16),
        in_specs=[hb] * len(args),
        out_specs=vm,
        scratch_shapes=scratch,
        compiler_params=pltpu.CompilerParams(
            collective_id=0, has_side_effects=True, vmem_limit_bytes=56 * 1024 * 1024
        ),
    )(*args)


def solution(mesh):
    return jax.shard_map(
        body,
        mesh=mesh,
        in_specs=(
            P("ep", None),
            P("ep", "tp"),
            P("ep", "tp"),
            P("ep", "tp"),
            P("ep", "tp", None, None),
            P("ep", "tp", None, None),
            P("ep", "tp", None),
            P("ep", "tp"),
            P("tp"),
            P("ep"),
            P("tp", None),
            P(),
            P(),
            P("ep", None),
            P("ep", None),
            P("ep", "tp", None),
            P("ep", "tp", None),
            P("ep", None, "tp"),
            P("tp", "ep"),
            P("tp", "ep"),
            P("ep", "tp"),
        ),
        out_specs=P("ep", "tp"),
        check_vma=False,
    )
```

```python
import functools
import math

import jax
import jax.numpy as jnp
from jax import lax
from jax.experimental import pallas as pl
from jax.experimental.pallas import tpu as pltpu
from jax.sharding import PartitionSpec as P

HEAD = 128
EPSILON = 1e-06
NC = 2
NY = 8
F32 = jnp.float32
BF16 = jnp.bfloat16


def dot(a, b):
    return jnp.dot(a, b, preferred_element_type=F32)


def dot_t(a, b):
    return lax.dot_general(a, b, (((1,), (1,)), ((), ())), preferred_element_type=F32)


ARGS = (
    ("resid", "q", "nk", "nv", "cg", "fl", "fb", "len", "rt", "rw", "gain", "mix")
    + ("k", "v", "wo", "wg", "wu", "wd", "dg", "du", "dd")
)


def kernel(dims, *refs):
    h = dict(zip(ARGS, refs))
    out_ref = refs[len(ARGS)]
    rest = refs[len(ARGS) + 1 :]
    local = dict(zip(ARGS[:18], rest))
    (codes, ct, dw, xbuf, st, rows, gts, pk, wmat, disp, er, psend, prec, hid) = rest[18:32]
    (psd, prd, hdd, dacc, osend, orecv, ret, rb, csend, cb) = rest[32:42]
    (lsem, xq, cq, wq, vq, yq, tq, zq, gq, pq, hq, aq, eq, sq, oq, bq) = rest[42:]
    NX, NZ, S, SLOTS, DX, CW, NCH, FD = dims
    NQ = NY * NC // 4
    ep = lax.axis_index("ep")
    t = lax.axis_index("tp")
    c = lax.rem(ep, NC)
    y = lax.rem(ep // NC, NY)
    z = ep // (NC * NY)
    q = y // 2
    o = 1 - c

    def dev(zz, yy, cc, xx):
        return ((zz * NY + yy) * NC + cc, xx)

    def remote(src, dst, sems, i, where):
        d = pltpu.make_async_remote_copy(
            src_ref=src,
            dst_ref=dst,
            send_sem=sems.at[(0, *i)],
            recv_sem=sems.at[(1, *i)],
            device_id=where,
            device_id_type=pl.DeviceIdType.MESH,
        )
        d.start()
        sent.append(d)
        return d

    sent = []
    xs = [lax.rem(t + d, NX) for d in range(NX)]
    xb = [lax.rem(t + NX - d, NX) for d in range(NX)]
    ys = [lax.rem(y + d, NY) for d in range(NY)]
    yb = [lax.rem(y + NY - d, NY) for d in range(NY)]
    zs = [lax.rem(z + d, NZ) for d in range(NZ)]
    zb = [lax.rem(z + NZ - d, NZ) for d in range(NZ)]

    def order(n):
        return sorted(range(1, n), key=lambda d: (min(d, n - d), d))

    loads = {}
    targets = dict(local, dg=dw.at[c, z, 0], du=dw.at[c, z, 1], dd=dw.at[c, z, 2])
    first = ["q", "k", "len", "cg", "fl", "fb", "nk", "nv", "dg", "du", "dd", "v", "wo"]
    first += ["rt", "rw", "resid", "gain", "mix"]
    for i, name in enumerate(first + [a for a in ARGS if a not in first]):
        loads[name] = pltpu.make_async_copy(h[name], targets[name], lsem.at[i])
        loads[name].start()

    partner = dev(z, y, o, t)
    barrier = pltpu.get_barrier_semaphore()
    peers = [dev(z, y, c, xs[d]) for d in range(1, NX)]
    peers += [dev(z, ys[d], c, t) for d in range(1, NY)]
    peers += [dev(zs[d], y, c, t) for d in range(1, NZ)]
    peers.append(partner)
    for p in peers:
        pl.semaphore_signal(barrier, inc=1, device_id=p, device_id_type=pl.DeviceIdType.MESH)

    def get(name):
        loads[name].wait()
        return local[name]

    tr = lax.broadcasted_iota(jnp.int32, (S, S), 0)
    tc = lax.broadcasted_iota(jnp.int32, (S, S), 1)

    def column(row):
        return jnp.sum(jnp.where(tr == tc, row, jnp.zeros_like(row)), axis=1, keepdims=True)

    lens = column(get("len")[...])
    cg_ref, fl_ref, fb_ref = get("cg"), get("fl"), get("fb")
    pos = lax.broadcasted_iota(jnp.int32, (S, SLOTS), 1)
    biases = []
    for j in range(2):
        cg = cg_ref[:, j, :]
        latest = jnp.sum(jnp.where(pos == lens - 1, cg, 0.0), axis=1, keepdims=True)
        pre = column(fl_ref[j : j + 1]) + fb_ref[0:1, j : j + 1]
        forget = jnp.minimum(pre, 0.0) - jnp.log(1.0 + jnp.exp(-jnp.abs(pre)))
        biases.append(jnp.where(pos < lens, latest + forget - cg, -jnp.inf))
    bias = jnp.concatenate(biases, axis=0)

    k_v = get("k")
    qq = get("q")[...]
    q2 = jnp.concatenate([qq[:, :HEAD], qq[:, HEAD:]], axis=0)
    rowid = lax.rem(lax.broadcasted_iota(jnp.int32, (2 * S, SLOTS), 0), S)
    raw = jnp.zeros((2 * S, SLOTS), F32)
    for s in range(S):
        part = dot_t(q2, k_v[s * SLOTS : (s + 1) * SLOTS, :])
        raw = jnp.where(rowid == s, part, raw)
    scale = 1.0 / math.sqrt(HEAD)
    scores = raw * scale + bias
    nk = get("nk")[...].astype(F32)
    nv = get("nv")[...].astype(F32)
    own = jnp.sum(q2.astype(F32) * jnp.concatenate([nk, nk], axis=0), axis=1, keepdims=True) * scale
    top = jnp.maximum(jnp.max(scores, axis=1, keepdims=True), own)
    past = jnp.exp(scores - top)
    wown = jnp.exp(own - top)
    total = jnp.sum(past, axis=1, keepdims=True) + wown
    probs = (past / total).astype(BF16).astype(F32)
    pown = (wown / total).astype(BF16).astype(F32)
    pl.semaphore_wait(barrier, len(peers))
    for name in ("dg", "du", "dd"):
        loads[name].wait()
    near = [d for d in order(NZ) if min(d, NZ - d) <= 2]
    w_cp, v_cp = {}, {}
    for d in near:
        w_cp[d] = remote(dw.at[c, z], dw.at[c, z], wq, (d,), dev(zs[d], y, c, t))
    v_cp[0] = remote(dw.at[c, z], dw.at[c, z], vq, (0,), partner)

    def pass_on(d):
        w_cp[d].wait_recv()
        if d == NZ // 2 and NZ == 8:
            w_cp[4, 1].wait_recv()
        v_cp[d] = remote(dw.at[c, zb[d]], dw.at[c, zb[d]], vq, (d,), partner)

    v_v = get("v")
    mixed = pown * jnp.concatenate([nv, nv], axis=0)
    for s in range(S):
        mixed = mixed + dot(
            jnp.where(rowid == s, probs, 0.0).astype(BF16), v_v[s * SLOTS : (s + 1) * SLOTS, :]
        )
    mixed = mixed.astype(BF16)
    attended = jnp.concatenate([mixed[:S], mixed[S:]], axis=1)
    wo_v = get("wo")
    for j in range(NX):
        xbuf[t, j] = dot(attended, wo_v[:, j * DX : (j + 1) * DX]).astype(BF16)
    x_cp, c_cp = {}, {}
    for d in order(NX)[::-1]:
        x_cp[d] = remote(xbuf.at[t], xbuf.at[t], xq, (d,), dev(z, y, c, xs[d]))

    rt = get("rt")[...].astype(F32)
    rw = get("rw")[...]
    lanes = lax.broadcasted_iota(jnp.int32, (S, NY * S), 1)
    place = lanes == y * S + lax.broadcasted_iota(jnp.int32, (S, NY * S), 0)
    for k in range(2):
        mine = column(rt[k : k + 1])
        rank = jnp.zeros((S, 1), F32)
        for i in range(2):
            taken = (rt[i : i + 1] == mine) & (tc < tr)
            rank = rank + jnp.sum(jnp.where(taken, 1.0, 0.0), axis=1, keepdims=True)
        code = 2.0 * mine + rank + 1.0
        codes[k : k + 1] = jnp.sum(jnp.where(place, code, 0.0), axis=0, keepdims=True)
        codes[2 + k : 3 + k] = jnp.sum(
            jnp.where(place, column(rw[k : k + 1]), 0.0), axis=0, keepdims=True
        )
    codes[4:8] = jnp.zeros((4, NY * S), F32)
    ct[y] = codes[...]

    for d in order(NY):
        c_cp[d] = remote(codes, ct.at[y], cq, (d,), dev(z, ys[d], c, t))

    for d in order(NY):
        c_cp[d].wait_recv()
    mine = jnp.sum(ct[...], axis=0)
    nslot = 2 * NY
    npick = NZ * nslot
    ntok = NY * S
    ii = lax.broadcasted_iota(jnp.int32, (npick, ntok), 0)
    tt = lax.broadcasted_iota(jnp.int32, (npick, ntok), 1)
    target = (2 * ((ii // nslot) * NQ + q) + lax.rem(ii // NY, 2) + 1).astype(F32)
    same = lax.rem(ii, NY) == tt // S
    hits = [(mine[k : k + 1] == target) & same for k in range(2)]
    pk[...] = jnp.where(hits[0] | hits[1], 1.0, 0.0).astype(BF16)
    wt = jnp.where(hits[0], mine[2:3], 0.0) + jnp.where(hits[1], mine[3:4], 0.0)
    wt = wt.T
    whi = wt.astype(BF16)
    wmat[:, 0:npick] = whi
    wmat[:, npick : 2 * npick] = (wt - whi.astype(F32)).astype(BF16)

    resid_ref, gain_ref, mix_ref = get("resid"), get("gain"), get("mix")
    def row_of(ref, j):
        n = DX // 128
        return jnp.concatenate(
            [ref[j * n + i : j * n + i + 1, :].astype(F32) for i in range(n)], axis=1
        )

    for d in order(NX):
        x_cp[d].wait_recv()
    sumsq = jnp.zeros((S, 1), F32)
    gsum = jnp.zeros((S, 1), F32)
    for j in range(NX):
        proj = xbuf[0, j].astype(F32)
        for i in range(1, NX):
            proj = proj + xbuf[i, j].astype(F32)
        state = resid_ref[:, j * DX : (j + 1) * DX].astype(F32) + proj.astype(BF16).astype(F32)
        sumsq = sumsq + jnp.sum(state * state, axis=1, keepdims=True)
        scaled = state * row_of(gain_ref, j)
        gsum = gsum + jnp.sum(scaled * row_of(mix_ref, j), axis=1, keepdims=True)
        st[0, j] = state
        st[1, j] = scaled
    inverse = lax.rsqrt(sumsq / (NX * DX) + EPSILON)
    gate = 1.0 / (1.0 + jnp.exp(-(inverse * gsum)))
    ghi = gate.astype(BF16).astype(F32)
    lane = lax.broadcasted_iota(jnp.int32, (S, 128), 1)
    rows[y] = (st[1, t] * inverse).astype(BF16)
    gts[y] = jnp.where(lane == 0, ghi, jnp.where(lane == 1, gate - ghi, 0.0)).astype(BF16)

    y_cp, t_cp = {}, {}
    for d in order(NY)[::-1]:
        y_cp[d] = remote(rows.at[y], rows.at[y], yq, (d,), dev(z, ys[d], c, t))

    for d in near:
        pass_on(d)
    if NZ == 8:
        for d, to in ((2, 1), (6, 7)):
            f = (to + d) % NZ
            w_cp[f] = remote(
                dw.at[c, zb[d]], dw.at[c, zb[d]], wq, (f,), dev(zs[to], y, c, t)
            )
        for i, d in enumerate((2, 6)):
            part = (c, zb[d], slice(None), slice(None), pl.ds(i * (DX // 2), DX // 2))
            f = remote(dw.at[part], dw.at[part], wq, (4 * (1 - i),), dev(zs[d], y, c, t))
            w_cp[(4, 1) if i else 4] = f
    far = [d for d in order(NZ) if d not in near]
    for d in order(NY):
        y_cp[d].wait_recv()

    own_rows = rows[...].reshape(ntok, DX)
    disp[...] = dot(pk[...], own_rows).astype(BF16).reshape(NZ, nslot, DX)
    er[c, z] = disp[z]
    z_cp, g_cp = {}, {}
    for d in order(NZ)[::-1]:
        z_cp[d] = remote(disp.at[zs[d]], er.at[c, z], zq, (d,), dev(zs[d], y, c, t))
    for d in order(NY):
        t_cp[d] = remote(gts.at[y], gts.at[y], tq, (d,), dev(z, ys[d], c, t))
    g_cp[0] = remote(disp.at[z], er.at[c, z], gq, (0,), partner)

    part = npick // NX
    p_cp, h_cp = {}, {}

    def scatter(half, j):
        rows_in = er[(c, o)[half]].reshape(npick, DX)
        for i, w in enumerate((wg_v, wu_v)):
            psend[half, j, :, :, i * CW : (i + 1) * CW] = (
                dot(rows_in, w[:, j * CW : (j + 1) * CW]).astype(BF16).reshape(NX, part, CW)
            )
        for d in order(NX)[::-1]:
            key = (half, j, d - 1)
            p_cp[key] = remote(
                psend.at[half, j, xs[d]], prec.at[key], pq, key, dev(z, y, c, xs[d])
            )

    def hidden(j):
        for half in range(2):
            acc = psend[half, j, t].astype(F32)
            for d in order(NX):
                p_cp[half, j, d - 1].wait_recv()
            for d in range(1, NX):
                acc = acc + prec[half, j, d - 1].astype(F32)
            hid[j, t, half] = swish(acc, CW)
        for d in order(NX)[::-1]:
            h_cp[j, d] = remote(
                hid.at[j, t], hid.at[j, t], hq, (j, d - 1), dev(z, y, c, xs[d])
            )

    def swish(acc, n):
        g, u = acc[:, :n], acc[:, n:]
        return (g / (1.0 + jnp.exp(-g)) * u).astype(BF16)

    for d in far:
        pass_on(d)

    for d in range(NZ):
        v_cp[d].wait_recv()

    nden = NC * NZ * FD
    dgw, duw, ddw = [
        dw[:, :, i].astype(F32).reshape(nden, DX).astype(BF16) for i in range(3)
    ]
    dchunk = ntok // NX
    psd[:, :, 0:nden] = dot_t(own_rows, dgw).astype(BF16).reshape(NX, dchunk, nden)
    psd[:, :, nden : 2 * nden] = dot_t(own_rows, duw).astype(BF16).reshape(NX, dchunk, nden)
    a_cp, e_cp = {}, {}
    for d in order(NX)[::-1]:
        a_cp[d] = remote(psd.at[xs[d]], prd.at[d - 1], aq, (d,), dev(z, y, c, xs[d]))
    for d in order(NZ):
        z_cp[d].wait_recv()
        g_cp[d] = remote(er.at[c, zb[d]], er.at[c, zb[d]], gq, (d,), partner)
    wg_v, wu_v = get("wg"), get("wu")
    for j in range(NCH):
        scatter(0, j)

    for d in range(NZ):
        g_cp[d].wait_recv()
    for j in range(NCH):
        scatter(1, j)
    for j in range(NCH):
        hidden(j)
    acc = psd[t].astype(F32)
    for d in order(NX):
        a_cp[d].wait_recv()
        acc = acc + prd[d - 1].astype(F32)
    hdd[t] = swish(acc, nden)
    for d in order(NX)[::-1]:
        e_cp[d] = remote(hdd.at[t], hdd.at[t], eq, (d,), dev(z, y, c, xs[d]))
    wd_v = get("wd")

    def down(which, j):
        rows_in = hid[j, :, which].reshape(npick, CW)
        return dot(rows_in, wd_v[j * CW : (j + 1) * CW, :])

    for j in range(NCH):
        for d in order(NX):
            h_cp[j, d].wait_recv()
        if j == 0:
            theirs, ours = down(1, 0), down(0, 0)
        elif j < NCH - 1:
            theirs, ours = theirs + down(1, j), ours + down(0, j)
    if NCH > 1:
        theirs = theirs + down(1, NCH - 1)

    osend[...] = theirs.astype(BF16).reshape(NZ, nslot, DX)
    s_cp = remote(osend, orecv, sq, (0,), partner)
    if NCH > 1:
        ours = ours + down(0, NCH - 1)
    s_cp.wait_recv()
    ret[...] = (ours + orecv[...].reshape(npick, DX).astype(F32)).astype(BF16).reshape(
        NZ, nslot, DX
    )

    o_cp = {}
    for d in order(NZ)[::-1]:
        o_cp[d] = remote(ret.at[zs[d]], rb.at[z], oq, (d,), dev(zs[d], y, c, t))
    rb[z] = ret[z]
    for d in order(NY):
        t_cp[d].wait_recv()
    for d in order(NX):
        e_cp[d].wait_recv()
    gates = gts[...].reshape(ntok, 128)
    gates = gates[:, 0:1].astype(F32) + gates[:, 1:2].astype(F32)
    dacc[...] = gates * dot(hdd[...].reshape(ntok, nden), ddw)
    for d in order(NZ):
        o_cp[d].wait_recv()
    back = rb[...].reshape(npick, DX)
    both = jnp.concatenate([back, back], axis=0)
    comb = dot(wmat[...], both) + dacc[...]
    csend[...] = comb.astype(BF16).reshape(NY, S, DX)

    b_cp = {}
    for d in order(NY)[::-1]:
        b_cp[d] = remote(csend.at[ys[d]], cb.at[y], bq, (d,), dev(z, ys[d], c, t))
    cb[y] = csend[y]
    for d in order(NY):
        b_cp[d].wait_recv()
    res = st[0, t]
    for yy in range(NY):
        res = res + cb[yy].astype(F32)
    out_ref[...] = res.astype(BF16)
    for d in sent:
        d.wait_send()


def body(
    resid,
    queries,
    new_keys,
    new_values,
    key_cache,
    value_cache,
    cum_gate,
    forget_logit,
    forget_bias,
    lengths,
    out_weight,
    norm_gain,
    mix_vector,
    routes,
    route_weight,
    expert_gate,
    expert_up,
    expert_down,
    dense_gate,
    dense_up,
    dense_down,
):
    NX = lax.axis_size("tp")
    n_ep = lax.axis_size("ep")
    NZ = n_ep // (NC * NY)
    S, D = resid.shape
    SLOTS = key_cache.shape[2]
    DX = D // NX
    FF = expert_gate.shape[2]
    FD = dense_gate.shape[1]
    CW = min(256, FF)
    NCH = FF // CW
    dims = (NX, NZ, S, SLOTS, DX, CW, NCH, FD)
    nslot = 2 * NY
    npick = NZ * nslot
    ntok = NY * S
    nden = NC * NZ * FD
    part = npick // NX
    dchunk = ntok // NX
    vm = pl.BlockSpec(memory_space=pltpu.VMEM)
    hb = pl.BlockSpec(memory_space=pl.ANY)
    args = (
        resid,
        queries,
        new_keys,
        new_values,
        cum_gate,
        forget_logit.T,
        forget_bias.reshape(1, 2),
        lengths.reshape(1, S),
        routes.T,
        route_weight.T,
        norm_gain.reshape(D // 128, 128),
        mix_vector.reshape(D // 128, 128),
        key_cache.reshape(S * SLOTS, HEAD),
        value_cache.reshape(S * SLOTS, HEAD),
        out_weight,
        expert_gate[0],
        expert_up[0],
        expert_down[0],
        dense_gate.T,
        dense_up.T,
        dense_down,
    )
    scratch = [pltpu.VMEM(a.shape, a.dtype) for a in args[:18]]
    scratch += [
        pltpu.VMEM(*sd)
        for sd in (
            ((8, ntok), F32),
            ((NY, 8, ntok), F32),
            ((NC, NZ, 3, FD, DX), BF16),
            ((NX, NX, S, DX), BF16),
            ((2, NX, S, DX), F32),
            ((NY, S, DX), BF16),
            ((NY, S, 128), BF16),
            ((npick, ntok), BF16),
            ((ntok, 2 * npick), BF16),
            ((NZ, nslot, DX), BF16),
            ((NC, NZ, nslot, DX), BF16),
            ((2, NCH, NX, part, 2 * CW), BF16),
            ((2, NCH, NX - 1, part, 2 * CW), BF16),
            ((NCH, NX, 2, part, CW), BF16),
            ((NX, dchunk, 2 * nden), BF16),
            ((NX - 1, dchunk, 2 * nden), BF16),
            ((NX, dchunk, nden), BF16),
            ((ntok, DX), F32),
            ((NZ, nslot, DX), BF16),
            ((NZ, nslot, DX), BF16),
            ((NZ, nslot, DX), BF16),
            ((NZ, nslot, DX), BF16),
            ((NY, S, DX), BF16),
            ((NY, S, DX), BF16),
        )
    ]
    dma = pltpu.SemaphoreType.DMA
    scratch += [dma((len(args),))]
    scratch += [
        dma((2, *n))
        for n in (
            (NX,),
            (NY,),
            (NZ,),
            (NZ,),
            (NY,),
            (NY,),
            (NZ,),
            (NZ,),
            (2, NCH, NX - 1),
            (NCH, NX - 1),
            (NX,),
            (NX,),
            (1,),
            (NZ,),
            (NY,),
        )
    ]
    return pl.pallas_call(
        functools.partial(kernel, dims),
        name="layer",
        out_shape=pltpu.VMEM((S, DX), BF16),
        in_specs=[hb] * len(args),
        out_specs=vm,
        scratch_shapes=scratch,
        compiler_params=pltpu.CompilerParams(
            collective_id=0, has_side_effects=True, vmem_limit_bytes=56 * 1024 * 1024
        ),
    )(*args)


def solution(mesh):
    return jax.shard_map(
        body,
        mesh=mesh,
        in_specs=(
            P("ep", None),
            P("ep", "tp"),
            P("ep", "tp"),
            P("ep", "tp"),
            P("ep", "tp", None, None),
            P("ep", "tp", None, None),
            P("ep", "tp", None),
            P("ep", "tp"),
            P("tp"),
            P("ep"),
            P("tp", None),
            P(),
            P(),
            P("ep", None),
            P("ep", None),
            P("ep", "tp", None),
            P("ep", "tp", None),
            P("ep", None, "tp"),
            P("tp", "ep"),
            P("tp", "ep"),
            P("ep", "tp"),
        ),
        out_specs=P("ep", "tp"),
        check_vma=False,
    )
```
